512 devices in a mesh: ep: 128 (over z, x, core), tp: 4 (over y).
Axes of the slice: x: 4, y: 4, z: 16, core: 2. Of those that a mesh axis runs over, the one named last changes fastest.
Arguments:
- tokens: bfloat16 [16384, 1024], P('ep', 'tp'), may hold values from -6 to 6
- cotangent: bfloat16 [16384, 1024], P('ep', 'tp'), may hold values from -12 to 12
- routes: int32 [16384, 2], P('ep'), may hold values from 0 to 63, all different within a row; in each aligned block of 128 rows (0 to 127, 128 to 255, ...) at most 5 rows name the same one
- route_weights: bfloat16 [16384, 2], P('ep'), may hold values from 0.099609375 to 0.8984375
- w_gate: bfloat16 [128, 1024, 1408], P('ep', None, 'tp'), may hold values from -0.1875 to 0.1875
- w_up: bfloat16 [128, 1024, 1408], P('ep', None, 'tp'), may hold values from -0.1875 to 0.1875
- w_down: bfloat16 [128, 1408, 1024], P('ep', 'tp'), may hold values from -0.109375 to 0.109375
- dense_weight: bfloat16 [1024, 1024], P('tp', 'ep'), may hold values from -0.75 to 0.75
- mix_gate: float32 [1024], replicated, may hold values from 0.1 to 1.9
Outputs:
- token_grad: bfloat16 [16384, 1024], P('ep', 'tp')
- route_grad: float32 [16384, 2], P('ep')
- gate_grad: bfloat16 [128, 1024, 1408], P('ep', None, 'tp')
- up_grad: bfloat16 [128, 1024, 1408], P('ep', None, 'tp')
- down_grad: bfloat16 [128, 1408, 1024], P('ep', 'tp')
- dense_grad: float32 [1024, 1024], P('tp', 'ep')
- mix_grad: float32 [1024], replicated
The draws below stay inside these ranges and needn't reach their ends.
Inputs may be any that keep to these rules, and one draw needn't show every extreme that they name: `routes`: each row names 2 different experts. In the rows of one index of ep (aligned blocks of 128 rows) no expert is named by more than 5 rows, a bound that some block reaches.
All inputs are finite; a program needn't handle non-finite values.
Results may differ from the reference program's by a relative error of at most 0.0065.
Values may be sent and summed in bfloat16 or wider, within the bound.
No kernel may reach another device: no remote copies, remote signals or barrier semaphores. Data moves between devices by JAX's collectives and lax.ppermute only.
A program may use at most 64 MiB of HBM per device.

```python
import math
import jax
import jax.numpy as jnp
import numpy as np
from jax import lax

D = 1024
FF = 2816
TOP = 2
TOK_DEV = 128
GROUP = 2
EXPERTS = 64
CAP = 5
FFB = 1408
SLICE = 352
TOKENS = 16384
N_EP = 128
N_TP = 4


def strengthened(values, stream_key, source, target, shards_of, factor):
    owner, partner = [(jnp.arange(values.shape[axis_at]) // (values.shape[axis_at] // shards_of)).reshape([-1 if axis == axis_at else 1 for axis in range(values.ndim)]) for axis_at in (source, target)]
    chosen = jax.random.permutation(stream_key, shards_of)[partner]
    strong = (owner == chosen) | (owner == (partner + shards_of // 2) % shards_of)
    return jnp.where(strong, factor * values, values)


def block_scale(stream_key, dims, pieces, smallest, top_value):
    factor_of, own = 1.0, jax.random.fold_in(stream_key, 6)
    for dim, blocks in pieces:
        draws = jnp.exp(jax.random.uniform(jax.random.fold_in(own, dim), (blocks,), jnp.float32, smallest / len(pieces), top_value / len(pieces)))
        factor_of = factor_of * jnp.repeat(draws, dims[dim] // blocks).reshape([-1 if axis == dim else 1 for axis in range(len(dims))])
    return factor_of


def deal_out(own_key, own, number, rows, number_of, top, limit, lean):
    sequence = jax.random.permutation(own_key, number_of)
    packed, ordinary = shares(number_of, rows * top, limit, lean, True), shares(number_of, rows * top, limit, lean, False)
    places = jnp.arange(number_of)

    def named(sizes, offset_by):
        used = int((sizes > 0).sum())
        fixed = max(1, used // 4)
        passed = fixed + (places - fixed + offset_by * (used - fixed)) % max(1, number_of - fixed)
        return jnp.zeros((number_of,), jnp.int32).at[sequence[jnp.where(places < fixed, places, passed)]].set(jnp.asarray(sizes, jnp.int32))

    sizes = jnp.where(number % 4 == 0, named(packed, number // 4), named(ordinary, number - number // 4 - 1))
    mixed = jax.random.permutation(jax.random.fold_in(own, 3), number_of)
    donor, taker = mixed[0:number_of // 2 * 2:2], mixed[1:number_of // 2 * 2:2]
    room = jnp.minimum(sizes[donor] - 1, limit - sizes[taker]) // 2
    room = jnp.where((donor == sequence[0]) | (taker == sequence[0]) | (sizes[taker] == 0), 0, jnp.maximum(room, 0))
    passed = jax.random.randint(jax.random.fold_in(own, 4), (number_of // 2,), 0, 1 << 20) % (room + 1)
    sizes = sizes.at[donor].add(-passed).at[taker].add(passed)
    labels = jnp.searchsorted(jnp.cumsum(sizes), jnp.arange(rows * top), side="right").astype(jnp.int32)
    listing = labels.reshape(top, rows).T
    listing = listing[jax.random.permutation(jax.random.fold_in(own, 1), rows)]
    offset_by = jax.random.randint(jax.random.fold_in(own, 2), (rows, 1), 0, top)
    return jnp.take_along_axis(listing, (jnp.arange(top)[None, :] + offset_by) % top, axis=1)


def shares(amount, total, limit, lean, full):
    loads = [(1 << 20) // math.isqrt(rank ** lean) + 1 for rank in range(1, amount + 1)]
    largest = limit if full else min(limit, max(-(-total // amount), total * loads[0] // sum(loads)))
    least = 1 if total - largest >= amount - 1 else 0
    counts, surplus = [largest] + [least] * (amount - 1), total - largest - least * (amount - 1)
    while surplus > 0:
        movable = [i for i in range(1, amount) if counts[i] < largest] or [i for i in range(1, amount) if counts[i] < limit]
        mass, left = sum([loads[i] for i in movable]), surplus
        for i in movable:
            extra = min(limit - counts[i], max(1, left * loads[i] // mass), surplus)
            counts[i] = counts[i] + extra
            surplus = surplus - extra
    return np.array(counts)


def noise(key, dims, scale, most, shards=(), held_as=jnp.bfloat16):
    drawn = scale * jax.random.normal(key, dims, jnp.float32)
    if shards:
        drawn = drawn * block_scale(key, dims, shards, -0.22, 0.18)
    return jnp.clip(drawn, -most, most).astype(held_as)


def noise_with(own_key, extent, width, most, cuts, heavy, kind=jnp.bfloat16):
    values = width * jax.random.normal(own_key, extent, jnp.float32)
    if cuts:
        values = values * block_scale(own_key, extent, cuts, -0.22, 0.18)
    return jnp.clip(strengthened(values, jax.random.fold_in(own_key, 3), *heavy), -most, most).astype(kind)


def setup_inputs(seed: int = 0) -> dict:
    streams_of = jax.random.split(jax.random.key(seed), 10)
    tokens = noise(streams_of[0], (TOKENS, D), 1.0, 6.0, ((0, 128), (1, 4)))
    cotangent = noise_with(streams_of[1], (TOKENS, D), 0.5, 12.0, ((0, 128), (1, 4)), (0, 1, 128, 5.5))
    routes_keys = jax.random.split(jax.random.fold_in(streams_of[2], 1), TOKENS // TOK_DEV)
    routes_turns = jax.random.permutation(jax.random.fold_in(streams_of[2], 3), TOKENS // TOK_DEV)
    routes = jax.vmap(lambda own, number: deal_out(jax.random.fold_in(streams_of[2], 2), own, number, TOK_DEV, EXPERTS, TOP, CAP, 2))(routes_keys, routes_turns).reshape((TOKENS, TOP))
    route_weights = jnp.clip(0.099609375 + 0.7988281 * jax.random.uniform(streams_of[3], (TOKENS, TOP), jnp.float32) ** block_scale(streams_of[3], (TOKENS, TOP), ((0, 128),), -0.2, 0.2), 0.099609375, 0.8984375).astype(jnp.bfloat16)
    w_gate = noise(streams_of[4], (EXPERTS * GROUP, D, FFB), D ** -0.5, 0.1875, ((0, 128), (2, 4)))
    w_up = noise(streams_of[5], (EXPERTS * GROUP, D, FFB), D ** -0.5, 0.1875, ((0, 128), (2, 4)))
    w_down = noise(streams_of[6], (EXPERTS * GROUP, FFB, D), FF ** -0.5, 0.109375, ((0, 128), (1, 4)))
    dense_weight = noise_with(streams_of[7], (D, D), D ** -0.5, 0.75, ((0, 4), (1, 128)), (1, 0, 128, 5.5))
    mix_gate = jnp.clip(1.0 + 0.18 * jax.random.normal(streams_of[8], (D,), jnp.float32), 0.1, 1.9)
    return dict(tokens=tokens, cotangent=cotangent, routes=routes, route_weights=route_weights, w_gate=w_gate, w_up=w_up, w_down=w_down, dense_weight=dense_weight, mix_gate=mix_gate)


def reference(tokens, cotangent, routes, route_weights, w_gate, w_up, w_down, dense_weight, mix_gate):
    picks = TOK_DEV * TOP
    slots = EXPERTS * CAP
    blocked = routes.reshape(N_EP, picks)
    onehot = (blocked[:, :, None] == jnp.arange(EXPERTS, dtype=jnp.int32)[None, None, :]).astype(jnp.int32)
    ranking = jnp.cumsum(onehot, axis=1) - 1
    target = (blocked * CAP + jnp.sum(onehot * ranking, axis=2)).astype(jnp.int32)
    pick_index = jnp.arange(picks, dtype=jnp.int32)
    block_base = (jnp.arange(N_EP, dtype=jnp.int32) * TOK_DEV)[:, None]
    token_index = (block_base + pick_index[None, :] // TOP).astype(jnp.int32)
    block_rows = jnp.broadcast_to(jnp.arange(N_EP, dtype=jnp.int32)[:, None], target.shape)
    source = jnp.zeros((N_EP, slots), jnp.int32).at[block_rows, target].set(token_index)
    pick_slot = jnp.zeros((N_EP, slots), jnp.int32).at[block_rows, target].set(
        jnp.broadcast_to(pick_index[None, :] % TOP, target.shape).astype(jnp.int32))
    filled = jnp.zeros((N_EP, slots), jnp.float32).at[block_rows, target].set(1.0)
    slot_weight = jnp.zeros((N_EP, slots), jnp.float32).at[block_rows, target].set(
        route_weights.reshape(N_EP, picks).astype(jnp.float32))

    def by_expert(table):
        return table.reshape(N_EP, EXPERTS, CAP).transpose(1, 0, 2).reshape(EXPERTS, N_EP * CAP)

    gate_blocks = w_gate.reshape(EXPERTS, GROUP, D, FFB)
    up_blocks = w_up.reshape(EXPERTS, GROUP, D, FFB)
    down_blocks = w_down.reshape(EXPERTS, GROUP, FFB, D)
    slices = GROUP * N_TP

    def one_expert(carry, inputs):
        token_acc, route_acc = carry
        src, kslot, live, weight, gate_b, up_b, down_b = inputs
        token_rows = tokens[src]
        grad_rows = cotangent[src]
        gate_matrix = gate_b.transpose(1, 0, 2).reshape(D, FF)
        up_matrix = up_b.transpose(1, 0, 2).reshape(D, FF)
        down_matrix = down_b.reshape(FF, D)
        pre_gate = jnp.dot(token_rows, gate_matrix, preferred_element_type=jnp.float32)
        pre_up = jnp.dot(token_rows, up_matrix, preferred_element_type=jnp.float32)
        sigmoid_gate = jax.nn.sigmoid(pre_gate)
        activated = pre_gate * sigmoid_gate
        hidden = activated * pre_up
        hidden_bf = hidden.astype(jnp.bfloat16)
        projected = jnp.dot(grad_rows, down_matrix.T, preferred_element_type=jnp.float32)
        route_part = jnp.sum(hidden_bf.astype(jnp.float32) * projected, axis=1)
        weight_col = weight[:, None]
        hidden_grad = weight_col * projected
        d_gate = (hidden_grad * pre_up * sigmoid_gate * (1.0 + pre_gate * (1.0 - sigmoid_gate))).astype(jnp.bfloat16)
        d_up = (hidden_grad * activated).astype(jnp.bfloat16)
        weighted = (weight_col * hidden).astype(jnp.bfloat16)
        gate_delta = jnp.dot(token_rows.T, d_gate, preferred_element_type=jnp.float32).astype(jnp.bfloat16)
        up_delta = jnp.dot(token_rows.T, d_up, preferred_element_type=jnp.float32).astype(jnp.bfloat16)
        down_delta = jnp.dot(weighted.T, grad_rows, preferred_element_type=jnp.float32).astype(jnp.bfloat16)
        row_count = token_rows.shape[0]
        gate_slices = d_gate.astype(jnp.float32).reshape(row_count, slices, SLICE)
        up_slices = d_up.astype(jnp.float32).reshape(row_count, slices, SLICE)
        gate_cols = gate_matrix.astype(jnp.float32).reshape(D, slices, SLICE)
        up_cols = up_matrix.astype(jnp.float32).reshape(D, slices, SLICE)
        partial_value = (jnp.einsum('rsf,dsf->rsd', gate_slices, gate_cols)
                   + jnp.einsum('rsf,dsf->rsd', up_slices, up_cols)).astype(jnp.bfloat16)
        block_sum = jnp.sum(partial_value.reshape(row_count, GROUP, N_TP, D).astype(jnp.float32), axis=2).astype(jnp.bfloat16)
        summed = jnp.sum(block_sum.astype(jnp.float32), axis=1)
        token_acc = token_acc.at[src].add(summed * live[:, None])
        route_acc = route_acc.at[src, kslot].add(route_part * live)
        outputs = (gate_delta.reshape(D, GROUP, FFB).transpose(1, 0, 2),
                   up_delta.reshape(D, GROUP, FFB).transpose(1, 0, 2),
                   down_delta.reshape(GROUP, FFB, D))
        return (token_acc, route_acc), outputs

    start = (jnp.zeros((TOKENS, D), jnp.float32), jnp.zeros((TOKENS, TOP), jnp.float32))
    inputs = (by_expert(source), by_expert(pick_slot), by_expert(filled), by_expert(slot_weight),
              gate_blocks, up_blocks, down_blocks)
    (token_acc, route_acc), (gate_all, up_all, down_all) = lax.scan(one_expert, start, inputs)
    scaled = (mix_gate[None, :] * cotangent.astype(jnp.float32)).astype(jnp.bfloat16)
    dense_dx = jnp.dot(scaled, dense_weight.T, preferred_element_type=jnp.float32)
    token_grad = (token_acc + dense_dx).astype(jnp.bfloat16)
    dense_grad = jnp.dot(tokens.T, scaled, preferred_element_type=jnp.float32) / N_EP
    dense_out = jnp.dot(tokens, dense_weight, preferred_element_type=jnp.float32)
    mix_grad = jnp.sum(cotangent.astype(jnp.float32) * dense_out, axis=0) / N_EP
    gate_grad = gate_all.reshape(EXPERTS * GROUP, D, FFB)
    up_grad = up_all.reshape(EXPERTS * GROUP, D, FFB)
    down_grad = down_all.reshape(EXPERTS * GROUP, FFB, D)
    return token_grad, route_acc, gate_grad, up_grad, down_grad, dense_grad, mix_grad
```

```python
import jax
import jax.numpy as jnp
from jax import lax
from jax.experimental import pallas as pl
from jax.experimental.pallas import tpu as pltpu
from jax.sharding import Mesh
from jax.sharding import PartitionSpec as P

EP = ("ep_0", "ep_1", "ep_2")
CHIPS = ("ep_0", "ep_1")
F32 = jnp.float32
BF16 = jnp.bfloat16
EXPERTS = 64
CAP = 5
ROWS = EXPERTS * CAP
EXTRA = 16
TP = 4


def iota(shape, dim):
    return lax.broadcasted_iota(jnp.int32, shape, dim)


def dot(a, b):
    return jnp.dot(a, b, preferred_element_type=F32)


def dot_nt(a, b):
    return lax.dot_general(a, b, (((1,), (1,)), ((), ())), preferred_element_type=F32)


def dot_tn(a, b):
    return lax.dot_general(a, b, (((0,), (0,)), ((), ())), preferred_element_type=F32)


def onehot(cond):
    return jnp.where(cond, 1.0, 0.0).astype(BF16)


def call(kernel, outs, *args):
    return pl.pallas_call(
        kernel,
        out_shape=outs,
        compiler_params=pltpu.CompilerParams(vmem_limit_bytes=48 * 1024 * 1024),
    )(*args)


def pack_kernel(routes_ref, weights_ref, tok_ref, cot_ref, out_ref, keys_ref, cols_ref):
    tokens = 128
    r0 = routes_ref[0:1, :].astype(F32)
    r1 = routes_ref[1:2, :].astype(F32)
    w = weights_ref[...].astype(F32)
    row = iota((tokens, tokens), 0)
    lane = iota((tokens, tokens), 1)
    eye = row == lane

    def to_col(v):
        return jnp.sum(jnp.where(eye, v, 0.0), axis=1, keepdims=True)

    c0 = to_col(r0)
    c1 = to_col(r1)
    before = row < lane

    def rank_of(r):
        hit = jnp.where(c0 == r, 1.0, 0.0) + jnp.where(c1 == r, 1.0, 0.0)
        return jnp.sum(jnp.where(before, hit, 0.0), axis=0, keepdims=True)

    k0 = rank_of(r0)
    k1 = rank_of(r1)
    four = jnp.concatenate([(r0 * CAP + k0) * 4 + i for i in range(4)], axis=1)
    four_b = jnp.concatenate([(r1 * CAP + k1) * 4 + i for i in range(4)], axis=1)
    msgs = EXPERTS * 8
    m_row = iota((msgs, 512), 0)
    dest = m_row // 8
    sub = m_row % 8
    data = jnp.concatenate(
        [tok_ref[:, :128], tok_ref[:, 128:], cot_ref[:, :128], cot_ref[:, 128:]], axis=0
    )
    for j in range(3):
        cell = j * 8 + sub
        key = jnp.where(cell < 20, dest * 20 + cell, -1).astype(F32)
        block = dot(onehot((key == four) | (key == four_b)), data)
        if j == 2:
            both = jnp.concatenate([r0, r1], axis=1)
            there = onehot((m_row[:, :256].astype(F32) == both * 8 + 4))
            lane_f = lane.astype(F32)
            v0 = jnp.where(lane_f == to_col(k0), to_col(w[0:1, :]), 0.0)
            v1 = jnp.where(lane_f == to_col(k1), to_col(w[1:2, :]), 0.0)
            block = block + dot(there, jnp.concatenate([v0, v1], axis=0).astype(BF16))
        out_ref[:, j * 128 : (j + 1) * 128] = block.astype(BF16)
    eight = iota((8, tokens), 0)
    keys_ref[...] = jnp.where(
        eight == 0, r0, jnp.where(eight == 1, r1, jnp.where(eight == 2, k0, k1))
    )
    cols_ref[...] = jnp.where(
        lane == 0, to_col(r0 * 8 + k0), jnp.where(lane == 1, to_col(r1 * 8 + k1), 0.0)
    )


def unpack_kernel(in_ref, out_ref):
    msgs = EXPERTS * 8
    p_row = iota((512, msgs), 0)
    p_col = iota((512, msgs), 1)
    chunk = p_row // 128
    half = (p_row % 128) // 64
    src = p_row % 64
    perm = onehot(p_col == src * 8 + half * 4 + chunk)
    rows = dot(perm, in_ref[...])
    by_src = rows[64:128, 256:384]
    tall = jnp.concatenate([by_src] * CAP, axis=0)
    t_row = iota((ROWS, 128), 0)
    t_lane = iota((ROWS, 128), 1)
    tall = jnp.where(t_row // 64 == t_lane, tall, 0.0).astype(BF16)
    w_row = dot_nt(jnp.full((EXTRA, 128), 1.0, BF16), tall).astype(BF16)
    rows = rows.astype(BF16)
    for t in range(TP):
        for c in range(4):
            for j in range(3):
                n = 128 if j < 2 else 64
                out_ref[t, j * 128 : j * 128 + n, c * 128 : (c + 1) * 128] = rows[
                    c * 128 : c * 128 + n, j * 128 : (j + 1) * 128
                ]
        out_ref[t, ROWS : ROWS + EXTRA, :] = jnp.zeros((EXTRA, 512), BF16)
        out_ref[t, ROWS : ROWS + EXTRA, 0:ROWS] = w_row


def expert_kernel(in_ref, wg_ref, wu_ref, wd_ref, z_ref, dg_ref, du_ref, wt_ref):
    def summed(lo, w_ref):
        return sum(
            dot_nt(in_ref[t, 0:ROWS, lo : lo + 256], w_ref[:, t * 256 : (t + 1) * 256])
            for t in range(TP)
        )

    pre_gate = summed(0, wg_ref)
    pre_up = summed(0, wu_ref)
    projected = summed(256, wd_ref)
    w_row = in_ref[0, ROWS : ROWS + EXTRA, 0:ROWS].astype(F32)[0:1, :]
    eye = iota((ROWS, ROWS), 0) == iota((ROWS, ROWS), 1)
    weight = jnp.sum(jnp.where(eye, w_row, 0.0), axis=1, keepdims=True)
    sig = jax.nn.sigmoid(pre_gate)
    activated = pre_gate * sig
    hidden = activated * pre_up
    route = jnp.sum(hidden.astype(BF16).astype(F32) * projected, axis=1, keepdims=True)
    grad = weight * projected
    d_gate = (grad * pre_up * sig * (1.0 + pre_gate * (1.0 - sig))).astype(BF16)
    d_up = (grad * activated).astype(BF16)
    dg_ref[...] = d_gate
    du_ref[...] = d_up
    wt_ref[...] = (weight * hidden).astype(BF16)
    part = (dot(d_gate, wg_ref[...]) + dot(d_up, wu_ref[...])).astype(BF16)
    hi = route.astype(BF16).astype(F32)
    lo = route - hi
    lane = iota((ROWS, 128), 1)
    pair = jnp.where(lane == 0, hi, jnp.where(lane == 1, lo, 0.0))
    pair = jnp.concatenate([pair, jnp.zeros((512 - ROWS, 128), F32)], axis=0).astype(BF16)
    pick = onehot(iota((EXTRA, 128), 0) == iota((EXTRA, 128), 1))
    flat = dot_nt(pick, pair)
    extra = jnp.concatenate([flat[0:8, 0:256], flat[0:8, 256:512]], axis=0).astype(BF16)
    for t in range(TP):
        z_ref[t, 0:ROWS, :] = part[:, t * 256 : (t + 1) * 256]
        z_ref[t, ROWS : ROWS + EXTRA, :] = extra


def return_kernel(in_ref, mix_ref, out_ref):
    total = sum(in_ref[t].astype(F32) for t in range(TP))
    msgs = EXPERTS * 8
    rows = total[0:ROWS].astype(BF16)
    m_row = iota((msgs, 512), 0)
    m_col = iota((msgs, 512), 1)
    dest = m_row // 8
    sub = m_row % 8
    perm = onehot((m_col == sub * 64 + dest) & (sub < CAP))
    out = dot(perm[:, 0:ROWS], rows)
    first = total[ROWS : ROWS + 1] + total[ROWS + 1 : ROWS + 2]
    second = total[ROWS + 8 : ROWS + 9] + total[ROWS + 9 : ROWS + 10]
    route = jnp.concatenate([first, second], axis=1)
    hi = route.astype(BF16).astype(F32)
    lo = route - hi
    mine = (sub == CAP) & (m_col % 64 == dest)
    b_row = iota((512, 256), 0)
    b_col = iota((512, 256), 1)
    out = out + dot(jnp.where(mine, hi, 0.0).astype(BF16), onehot(b_row // 64 == b_col))
    out = out + dot(jnp.where(mine, lo, 0.0).astype(BF16), onehot(b_row // 64 == b_col - 128))
    out_sub = iota((msgs, 256), 0) % 8
    out = jnp.where(out_sub == CAP + 1, mix_ref[...], out)
    out_ref[...] = out.astype(BF16)


def final_kernel(in_ref, keys_ref, cols_ref, dense_ref, tok_ref, route_ref, mix_ref):
    msgs = EXPERTS * 8
    got = in_ref[...]
    lane = iota((128, msgs), 1).astype(F32)
    take = onehot((lane == cols_ref[:, 0:1]) | (lane == cols_ref[:, 1:2]))
    tok_ref[...] = (dot(take, got) + dense_ref[...]).astype(BF16)
    m_row = iota((msgs, 128), 0).astype(F32)
    l_row = iota((256, 128), 0).astype(F32)
    for a in range(2):
        expert = keys_ref[a : a + 1, :]
        rank = keys_ref[a + 2 : a + 3, :]
        cells = dot_tn(got, onehot(m_row == expert * 8 + CAP))
        keep = (l_row == rank) | (l_row == rank + 128)
        route_ref[a : a + 1, :] = jnp.sum(jnp.where(keep, cells, 0.0), axis=0, keepdims=True)
    e_row = iota((EXPERTS, msgs), 0)
    e_col = iota((EXPERTS, msgs), 1)
    mix = dot(onehot(e_col == e_row * 8 + CAP + 1), got)
    mix_ref[...] = mix[:, 0:128] + mix[:, 128:256]


def swap(value, axes):
    return lax.all_to_all(value, axes, split_axis=0, concat_axis=0, tiled=True)


def copies(value, n):
    return jnp.broadcast_to(value[None], (n,) + value.shape)


def local(tokens, cotangent, routes, route_weights, w_gate, w_up, w_down, dense_weight, mix_gate):
    ep_count = lax.axis_size(EP)
    wg = w_gate[0].T
    wu = w_up[0].T
    wd = w_down[0]
    dense_t = dense_weight.T
    packed, keys, cols = call(
        pack_kernel,
        (
            jax.ShapeDtypeStruct((512, 384), BF16),
            jax.ShapeDtypeStruct((8, 128), F32),
            jax.ShapeDtypeStruct((128, 128), F32),
        ),
        routes.T,
        route_weights.T,
        tokens,
        cotangent,
    )
    arrived = swap(packed.reshape(64, 8, 384), CHIPS)

    cot_all = swap(copies(cotangent, TP), "tp")
    moment = lax.dot_general(
        jnp.swapaxes(cot_all, 1, 2).reshape(1024, 128), tokens, (((1,), (0,)), ((), ())),
        preferred_element_type=F32,
    ).astype(BF16)
    moment = moment.reshape(16, 4, 2, 8, 256).transpose(2, 1, 0, 3, 4).reshape(2, 512, 256)
    moment = jnp.sum(swap(moment, "ep_2").astype(F32), axis=0).astype(BF16)
    moment = jnp.sum(swap(moment.reshape(4, 128, 256), "ep_1").astype(F32), axis=0).astype(BF16)
    both = jnp.concatenate([moment.reshape(16, 8, 256), copies(dense_t, 16)], axis=1)
    both = swap(both, "ep_0")
    moment = jnp.sum(both[:, 0:8].astype(F32), axis=0) * (1.0 / ep_count)
    gate = lax.dynamic_slice(mix_gate, (lax.axis_index(EP) * 8,), (8,))
    dense_grad = (moment * gate[:, None]).T
    share = jnp.sum(moment * dense_t.astype(F32), axis=1)
    share = jnp.pad(share[None, :], ((0, 0), (0, 120)))
    shares = swap(copies(share, 8), ("ep_2", "tp"))
    mix = jnp.sum(shares.reshape(2, TP, 128)[:, :, :8], axis=1).reshape(1, 16)
    mix_hi = mix.astype(BF16).astype(F32)
    mix_row = jnp.concatenate(
        [jnp.pad(mix_hi, ((0, 0), (0, 112))), jnp.pad(mix - mix_hi, ((0, 0), (0, 112)))], axis=1
    )
    dense_w = swap(copies(both[:, 8:16].reshape(128, 256), 4), "ep_1")
    dense_w = swap(copies(dense_w.reshape(512, 256), 2), "ep_2")
    dense_w = dense_w.reshape(2, 4, 16, 8, 256).transpose(2, 1, 0, 3, 4).reshape(TP, 256, 256)
    scaled = (mix_gate.reshape(TP, 1, 256) * cot_all.astype(F32)).astype(BF16)
    dense_dx = lax.dot_general(
        jnp.swapaxes(scaled, 0, 1).reshape(128, 1024), dense_w.reshape(1024, 256),
        (((1,), (0,)), ((), ())), preferred_element_type=F32,
    )

    own = call(
        unpack_kernel,
        jax.ShapeDtypeStruct((TP, ROWS + EXTRA, 512), BF16),
        arrived.reshape(512, 384),
    )
    own = swap(own, "tp")
    other = lax.ppermute(own, "ep_2", [(0, 1), (1, 0)])
    outs = (
        jax.ShapeDtypeStruct((TP, ROWS + EXTRA, 256), BF16),
        jax.ShapeDtypeStruct((ROWS, 352), BF16),
        jax.ShapeDtypeStruct((ROWS, 352), BF16),
        jax.ShapeDtypeStruct((ROWS, 352), BF16),
    )
    z_own, *act_own = call(expert_kernel, outs, own, wg, wu, wd)
    z_other, *act_other = call(expert_kernel, outs, other, wg, wu, wd)
    z_back = lax.ppermute(z_other, "ep_2", [(0, 1), (1, 0)])
    z_sum = (z_own.astype(F32) + z_back.astype(F32)).astype(BF16)
    z_all = swap(z_sum, "tp")
    back = call(return_kernel, jax.ShapeDtypeStruct((512, 256), BF16), z_all, mix_row)
    back = swap(back.reshape(64, 8, 256), CHIPS).reshape(512, 256)
    token_grad, route_t, mix_all = call(
        final_kernel,
        (
            jax.ShapeDtypeStruct((128, 256), BF16),
            jax.ShapeDtypeStruct((2, 128), F32),
            jax.ShapeDtypeStruct((EXPERTS, 128), F32),
        ),
        back,
        keys,
        cols,
        dense_dx,
    )
    mix_grad = mix_all[:, :16].reshape(1024)

    gate_grad, up_grad, down_grad = call(
        grads_kernel,
        tuple(jax.ShapeDtypeStruct((352, 1024), BF16) for _ in range(3)),
        own,
        other,
        *act_own,
        *act_other,
    )
    return (
        token_grad,
        route_t.T,
        gate_grad.T[None],
        up_grad.T[None],
        down_grad[None],
        dense_grad,
        mix_grad,
    )


def grads_kernel(own_ref, other_ref, dg0, du0, wt0, dg1, du1, wt1, gate_ref, up_ref, down_ref):
    for left0, left1, lo, out_ref in (
        (dg0, dg1, 0, gate_ref),
        (du0, du1, 0, up_ref),
        (wt0, wt1, 256, down_ref),
    ):
        left = jnp.concatenate([left0[...], left1[...]], axis=0)
        for t in range(TP):
            right = jnp.concatenate(
                [own_ref[t, 0:ROWS, lo : lo + 256], other_ref[t, 0:ROWS, lo : lo + 256]], axis=0
            )
            out_ref[:, t * 256 : (t + 1) * 256] = dot_tn(left, right).astype(BF16)


def solution(mesh):
    finer = Mesh(mesh.devices.reshape(16, 4, 2, mesh.shape["tp"]), ("ep_0", "ep_1", "ep_2", "tp"))
    in_specs = (
        P(EP, "tp"),
        P(EP, "tp"),
        P(EP, None),
        P(EP, None),
        P(EP, None, "tp"),
        P(EP, None, "tp"),
        P(EP, "tp", None),
        P("tp", EP),
        P(),
    )
    out_specs = (
        P(EP, "tp"),
        P(EP, None),
        P(EP, None, "tp"),
        P(EP, None, "tp"),
        P(EP, "tp", None),
        P("tp", EP),
        P(),
    )
    return jax.shard_map(local, mesh=finer, in_specs=in_specs, out_specs=out_specs, check_vma=False)
```

```python
import jax
import jax.numpy as jnp
from jax import lax
from jax.experimental import pallas as pl
from jax.experimental.pallas import tpu as pltpu
from jax.sharding import Mesh
from jax.sharding import PartitionSpec as P


EP = ("ep_0", "ep_1", "ep_2")
CHIPS = ("ep_0", "ep_1")
F32 = jnp.float32
BF16 = jnp.bfloat16
EXPERTS = 64
CAP = 5
ROWS = EXPERTS * CAP
EXTRA = 16
TP = 4


def iota(shape, dim):
    return lax.broadcasted_iota(jnp.int32, shape, dim)


def dot(a, b):
    return jnp.dot(a, b, preferred_element_type=F32)


def dot_nt(a, b):
    return lax.dot_general(a, b, (((1,), (1,)), ((), ())), preferred_element_type=F32)


def dot_tn(a, b):
    return lax.dot_general(a, b, (((0,), (0,)), ((), ())), preferred_element_type=F32)


def onehot(cond):
    return jnp.where(cond, 1.0, 0.0).astype(BF16)


def call(kernel, outs, *args, after=(), scratch=(), hbm=0, flops=0, out_specs=None):
    whole = pl.BlockSpec(memory_space=pltpu.VMEM)
    placed = pl.BlockSpec(memory_space=pl.ANY)
    in_hbm = pl.BlockSpec(memory_space=pltpu.HBM)
    count = len(args)

    def body(*refs):
        kernel(*refs[:count], *refs[count + len(after) :])

    return pl.pallas_call(
        body,
        out_shape=outs,
        in_specs=[in_hbm] * hbm + [whole] * (count - hbm) + [placed] * len(after),
        out_specs=out_specs or jax.tree.map(lambda _: whole, outs),
        scratch_shapes=list(scratch),
        cost_estimate=pl.CostEstimate(
            flops=flops or 200_000_000, bytes_accessed=1_000_000, transcendentals=0
        ),
        compiler_params=pltpu.CompilerParams(vmem_limit_bytes=20 * 1024 * 1024),
    )(*args, *after)


def struct(*shape, dtype=BF16):
    return jax.ShapeDtypeStruct(shape, dtype)


def pack_kernel(
    tok_hbm, cot_hbm, routes_ref, weights_ref, out_ref, keys_ref, cols_ref, cot_ref, tok_ref, sems
):
    tokens = 128
    tok_copy = pltpu.make_async_copy(tok_hbm, tok_ref, sems.at[0])
    cot_copy = pltpu.make_async_copy(cot_hbm, cot_ref, sems.at[1])
    tok_copy.start()
    cot_copy.start()
    r0 = routes_ref[0:1, :].astype(F32)
    r1 = routes_ref[1:2, :].astype(F32)
    w = weights_ref[...].astype(F32)
    row = iota((tokens, tokens), 0)
    lane = iota((tokens, tokens), 1)
    eye = row == lane

    def to_col(v):
        return jnp.sum(jnp.where(eye, v, 0.0), axis=1, keepdims=True)

    c0 = to_col(r0)
    c1 = to_col(r1)
    before = row < lane

    def rank_of(r):
        hit = jnp.where(c0 == r, 1.0, 0.0) + jnp.where(c1 == r, 1.0, 0.0)
        return jnp.sum(jnp.where(before, hit, 0.0), axis=0, keepdims=True)

    k0 = rank_of(r0)
    k1 = rank_of(r1)
    four = jnp.concatenate([(r0 * CAP + k0) * 4 + i for i in range(4)], axis=1)
    four_b = jnp.concatenate([(r1 * CAP + k1) * 4 + i for i in range(4)], axis=1)
    msgs = EXPERTS * 8
    m_row = iota((msgs, 512), 0)
    dest = m_row // 8
    sub = m_row % 8
    tok_copy.wait()
    cot_copy.wait()
    data = jnp.concatenate(
        [tok_ref[:, :128], tok_ref[:, 128:], cot_ref[:, :128], cot_ref[:, 128:]], axis=0
    )
    for j in range(3):
        cell = j * 8 + sub
        key = jnp.where(cell < 20, dest * 20 + cell, -1).astype(F32)
        block = dot(onehot((key == four) | (key == four_b)), data)
        if j == 2:
            both = jnp.concatenate([r0, r1], axis=1)
            there = onehot((m_row[:, :256].astype(F32) == both * 8 + 4))
            lane_f = lane.astype(F32)
            v0 = jnp.where(lane_f == to_col(k0), to_col(w[0:1, :]), 0.0)
            v1 = jnp.where(lane_f == to_col(k1), to_col(w[1:2, :]), 0.0)
            block = block + dot(there, jnp.concatenate([v0, v1], axis=0).astype(BF16))
        out_ref[:, j * 128 : (j + 1) * 128] = block.astype(BF16)
    eight = iota((8, tokens), 0)
    keys_ref[...] = jnp.where(
        eight == 0, r0, jnp.where(eight == 1, r1, jnp.where(eight == 2, k0, k1))
    )
    cols_ref[...] = jnp.where(
        lane == 0, to_col(r0 * 8 + k0), jnp.where(lane == 1, to_col(r1 * 8 + k1), 0.0)
    )


def unpack_kernel(in_ref, out_ref):
    msgs = EXPERTS * 8
    p_row = iota((512, msgs), 0)
    p_col = iota((512, msgs), 1)
    chunk = p_row // 128
    half = (p_row % 128) // 64
    src = p_row % 64
    perm = onehot(p_col == src * 8 + half * 4 + chunk)
    rows = dot(perm, in_ref[...])
    by_src = rows[64:128, 256:384]
    tall = jnp.concatenate([by_src] * CAP, axis=0)
    t_row = iota((ROWS, 128), 0)
    t_lane = iota((ROWS, 128), 1)
    tall = jnp.where(t_row // 64 == t_lane, tall, 0.0).astype(BF16)
    w_row = dot_nt(jnp.full((EXTRA, 128), 1.0, BF16), tall).astype(BF16)
    rows = rows.astype(BF16)
    for t in range(TP):
        for c in range(4):
            for j in range(3):
                n = 128 if j < 2 else 64
                out_ref[t, j * 128 : j * 128 + n, c * 128 : (c + 1) * 128] = rows[
                    c * 128 : c * 128 + n, j * 128 : (j + 1) * 128
                ]
        out_ref[t, ROWS : ROWS + EXTRA, :] = jnp.zeros((EXTRA, 512), BF16)
        out_ref[t, ROWS : ROWS + EXTRA, 0:ROWS] = w_row


def expert_kernel(
    in_hbm, wg_hbm, wu_hbm, wd_hbm, z_ref, dg_out, du_out, wt_out,
    in_ref, wg_ref, wu_ref, wd_ref, dg_ref, du_ref, wt_ref, sems,
):
    inward = [
        pltpu.make_async_copy(src, dst, sems.at[n])
        for n, (src, dst) in enumerate(
            ((in_hbm, in_ref), (wg_hbm, wg_ref), (wu_hbm, wu_ref), (wd_hbm, wd_ref))
        )
    ]
    outward = [
        pltpu.make_async_copy(src, dst, sems.at[4 + n])
        for n, (src, dst) in enumerate(((dg_ref, dg_out), (du_ref, du_out), (wt_ref, wt_out)))
    ]
    for copy in inward:
        copy.start()
    inward[0].wait()
    inward[1].wait()

    def summed(lo, w_ref):
        return sum(
            dot_nt(in_ref[t, 0:ROWS, lo : lo + 256], w_ref[:, t * 256 : (t + 1) * 256])
            for t in range(TP)
        )

    pre_gate = summed(0, wg_ref)
    inward[2].wait()
    pre_up = summed(0, wu_ref)
    inward[3].wait()
    projected = summed(256, wd_ref)
    w_row = in_ref[0, ROWS : ROWS + EXTRA, 0:ROWS].astype(F32)[0:1, :]
    eye = iota((ROWS, ROWS), 0) == iota((ROWS, ROWS), 1)
    weight = jnp.sum(jnp.where(eye, w_row, 0.0), axis=1, keepdims=True)
    sig = jax.nn.sigmoid(pre_gate)
    activated = pre_gate * sig
    hidden = activated * pre_up
    route = jnp.sum(hidden.astype(BF16).astype(F32) * projected, axis=1, keepdims=True)
    grad = weight * projected
    d_gate = (grad * pre_up * sig * (1.0 + pre_gate * (1.0 - sig))).astype(BF16)
    d_up = (grad * activated).astype(BF16)
    dg_ref[...] = d_gate
    du_ref[...] = d_up
    wt_ref[...] = (weight * hidden).astype(BF16)
    for copy in outward:
        copy.start()
    part = (dot(d_gate, wg_ref[...]) + dot(d_up, wu_ref[...])).astype(BF16)
    hi = route.astype(BF16).astype(F32)
    lo = route - hi
    lane = iota((ROWS, 128), 1)
    pair = jnp.where(lane == 0, hi, jnp.where(lane == 1, lo, 0.0))
    pair = jnp.concatenate([pair, jnp.zeros((512 - ROWS, 128), F32)], axis=0).astype(BF16)
    pick = onehot(iota((EXTRA, 128), 0) == iota((EXTRA, 128), 1))
    flat = dot_nt(pick, pair)
    extra = jnp.concatenate([flat[0:8, 0:256], flat[0:8, 256:512]], axis=0).astype(BF16)
    for t in range(TP):
        z_ref[t, 0:ROWS, :] = part[:, t * 256 : (t + 1) * 256]
        z_ref[t, ROWS : ROWS + EXTRA, :] = extra
    for copy in outward:
        copy.wait()


def return_kernel(in_ref, m0_ref, m1_ref, m2_ref, m3_ref, out_ref):
    total = sum(in_ref[t].astype(F32) for t in range(TP))
    msgs = EXPERTS * 8
    rows = total[0:ROWS].astype(BF16)
    m_row = iota((msgs, 512), 0)
    m_col = iota((msgs, 512), 1)
    dest = m_row // 8
    sub = m_row % 8
    perm = onehot((m_col == sub * 64 + dest) & (sub < CAP))
    out = dot(perm[:, 0:ROWS], rows)
    first = total[ROWS : ROWS + 1] + total[ROWS + 1 : ROWS + 2]
    second = total[ROWS + 8 : ROWS + 9] + total[ROWS + 9 : ROWS + 10]
    route = jnp.concatenate([first, second], axis=1)
    hi = route.astype(BF16).astype(F32)
    lo = route - hi
    mine = (sub == CAP) & (m_col % 64 == dest)
    b_row = iota((512, 256), 0)
    b_col = iota((512, 256), 1)
    out = out + dot(jnp.where(mine, hi, 0.0).astype(BF16), onehot(b_row // 64 == b_col))
    out = out + dot(jnp.where(mine, lo, 0.0).astype(BF16), onehot(b_row // 64 == b_col - 128))
    came = [m_ref[0:1, :] for m_ref in (m0_ref, m1_ref, m2_ref, m3_ref)]
    here = lax.axis_index("tp")
    mix = jnp.zeros((1, 128), F32)
    for t in range(TP):
        back = lax.rem(here - t + TP, TP)
        pick = came[3]
        for n in range(3):
            pick = jnp.where(back == n, came[n], pick)
        mix = mix + pick
    mix_hi = mix.astype(BF16).astype(F32)
    mix_row = jnp.concatenate([mix_hi, mix - mix_hi], axis=1)
    out_sub = iota((msgs, 256), 0) % 8
    out = jnp.where(out_sub == CAP + 1, mix_row, out)
    out_ref[...] = out.astype(BF16)


def final_kernel(in_ref, keys_ref, cols_ref, dense_ref, tok_ref, route_ref, mix_ref):
    msgs = EXPERTS * 8
    got = in_ref[...]
    lane = iota((128, msgs), 1).astype(F32)
    take = onehot((lane == cols_ref[:, 0:1]) | (lane == cols_ref[:, 1:2]))
    tok_ref[...] = (dot(take, got) + dense_ref[...]).astype(BF16)
    m_row = iota((msgs, 128), 0).astype(F32)
    l_row = iota((256, 128), 0).astype(F32)
    for a in range(2):
        expert = keys_ref[a : a + 1, :]
        rank = keys_ref[a + 2 : a + 3, :]
        cells = dot_tn(got, onehot(m_row == expert * 8 + CAP))
        keep = (l_row == rank) | (l_row == rank + 128)
        route_ref[a : a + 1, :] = jnp.sum(jnp.where(keep, cells, 0.0), axis=0, keepdims=True)
    e_row = iota((EXPERTS, msgs), 0)
    e_col = iota((EXPERTS, msgs), 1)
    mix = dot(onehot(e_col == e_row * 8 + CAP + 1), got)
    mix_ref[...] = mix[:, 0:128] + mix[:, 128:256]


def moment_kernel(cot_ref, tok_ref, keep_ref, send_ref):
    moment = dot_tn(cot_ref[...], tok_ref[...])
    north = lax.axis_index("ep_2") == 1
    for x in range(4):
        parts = []
        for c in range(2):
            starts = [(z * 8 + x * 2 + c) * 8 for z in range(16)]
            parts.append(jnp.concatenate([moment[s : s + 8] for s in starts], axis=0))
        span = slice(x * 128, (x + 1) * 128)
        keep_ref[span, :] = jnp.where(north, parts[1], parts[0])
        send_ref[span, :] = jnp.where(north, parts[0], parts[1]).astype(BF16)


def core_sum_kernel(keep_ref, got_ref, own_ref, s1_ref, s2_ref, s3_ref, sum_ref):
    sum_ref[...] = keep_ref[...] + got_ref[...].astype(F32)
    here = lax.axis_index("ep_1")

    def part(shift):
        start = pl.multiple_of(lax.rem(here + shift, 4) * 128, 128)
        return sum_ref[pl.ds(start, 128), :]

    own_ref[...] = part(0)
    s1_ref[...] = part(1).astype(BF16)
    s2_ref[...] = part(2).astype(BF16)
    s3_ref[...] = part(3).astype(BF16)


def x_sum_kernel(own_ref, r1_ref, r2_ref, r3_ref, dense_ref, out_ref):
    total = own_ref[...] + r1_ref[...].astype(F32)
    total = total + (r2_ref[...].astype(F32) + r3_ref[...].astype(F32))
    dense = dense_ref[...].astype(F32)
    pieces = []
    for z in range(16):
        pieces += [total[z * 8 : z * 8 + 8], dense]
    out_ref[...] = jnp.concatenate(pieces, axis=0).astype(BF16)


def z_sum_kernel(in_ref, gate_ref, dense_ref, grad_ref, share_ref, w_ref):
    got = in_ref[...].astype(F32)
    moment = sum(got[z * 16 : z * 16 + 8] for z in range(16)) * (1.0 / 128)
    w_ref[...] = jnp.concatenate(
        [got[z * 16 + 8 : z * 16 + 16] for z in range(16)], axis=0
    ).astype(BF16)
    core = lax.axis_index("ep_2")
    first = (lax.axis_index("ep_0") * 8 + lax.axis_index("ep_1") * 2 + core) * 8
    at = iota((8, 1024), 1) == first + iota((8, 1024), 0)
    gate = jnp.sum(jnp.where(at, gate_ref[...], 0.0), axis=1, keepdims=True)
    grad_ref[...] = moment * gate
    share = jnp.sum(moment * dense_ref[...].astype(F32), axis=1, keepdims=True)
    spot = iota((8, 128), 1) == core * 8 + iota((8, 128), 0)
    row = jnp.sum(jnp.where(spot, share, 0.0), axis=0, keepdims=True)
    share_ref[...] = jnp.broadcast_to(row, (8, 128))


def dense_kernel(cot_ref, gate_ref, own_ref, other_ref, out_ref):
    north = lax.axis_index("ep_2") == 1
    own = own_ref[...].astype(F32)
    other = other_ref[...].astype(F32)
    south_w = jnp.where(north, other, own)
    north_w = jnp.where(north, own, other)
    pieces = []
    for z in range(16):
        for x in range(4):
            s = (x * 16 + z) * 8
            pieces += [south_w[s : s + 8], north_w[s : s + 8]]
    weight = jnp.concatenate(pieces, axis=0).astype(BF16)
    scaled = (gate_ref[...] * cot_ref[...].astype(F32)).astype(BF16)
    out_ref[...] = dot(scaled, weight)


def add_kernel(a_ref, b_ref, out_ref):
    out_ref[...] = (a_ref[...].astype(F32) + b_ref[...].astype(F32)).astype(BF16)


def share_kernel(a_ref, b_ref, out_ref):
    out_ref[...] = a_ref[...] + b_ref[...]


def in_place(*arrays):
    return [pltpu.with_memory_space_constraint(a, pltpu.HBM) for a in arrays]


def swap(value, axes):
    return lax.all_to_all(value, axes, split_axis=0, concat_axis=0, tiled=True)


def shift(value, axis, by):
    n = lax.axis_size(axis)
    return lax.ppermute(value, axis, [(i, (i + by) % n) for i in range(n)])


def local(tokens, cotangent, routes, route_weights, w_gate, w_up, w_down, dense_weight, mix_gate):
    wg = w_gate[0].T
    wu = w_up[0].T
    wd = w_down[0]
    dense_t = dense_weight.T
    gate_row = mix_gate[None, :]
    tokens, cotangent, wg, wu, wd, routes_t, weights_t = in_place(
        tokens, cotangent, wg, wu, wd, routes.T, route_weights.T
    )
    packed, keys, cols, cot_here = call(
        pack_kernel,
        (
            struct(512, 384),
            struct(8, 128, dtype=F32),
            struct(128, 128, dtype=F32),
            struct(128, 256),
        ),
        tokens,
        cotangent,
        routes_t,
        weights_t,
        hbm=2,
        scratch=(
            pltpu.VMEM((128, 256), BF16),
            pltpu.SemaphoreType.DMA((2,)),
        ),
    )
    arrived = swap(packed.reshape(64, 8, 384), CHIPS)

    cot_all = lax.all_gather(cot_here, "tp", axis=1, tiled=True)
    keep, send = call(
        moment_kernel, (struct(512, 256, dtype=F32), struct(512, 256)), cot_all, tokens
    )
    here, *away = call(
        core_sum_kernel,
        (struct(128, 256, dtype=F32),) + (struct(128, 256),) * 3,
        keep,
        shift(send, "ep_2", 1),
        scratch=(pltpu.VMEM((512, 256), F32),),
    )
    both = call(
        x_sum_kernel,
        struct(256, 256),
        here,
        *(shift(piece, "ep_1", i + 1) for i, piece in enumerate(away)),
        dense_t,
    )

    own = call(
        unpack_kernel, struct(TP, ROWS + EXTRA, 512), arrived.reshape(512, 384), after=(here,)
    )
    own, both = lax.optimization_barrier((swap(own, "tp"), both))
    other = shift(own, "ep_2", 1)
    outs = (struct(TP, ROWS + EXTRA, 256),) + (pltpu.HBM((ROWS, 352), BF16),) * 3
    hbm_spec = pl.BlockSpec(memory_space=pltpu.HBM)
    vmem_spec = pl.BlockSpec(memory_space=pltpu.VMEM)
    expert = dict(
        hbm=4,
        flops=1_150_000_000,
        out_specs=(vmem_spec,) + (hbm_spec,) * 3,
        scratch=(pltpu.VMEM((TP, ROWS + EXTRA, 512), BF16),)
        + (pltpu.VMEM((352, 1024), BF16),) * 3
        + (pltpu.VMEM((ROWS, 352), BF16),) * 3
        + (pltpu.SemaphoreType.DMA((7,)),),
    )
    z_own, *act_own = call(expert_kernel, outs, own, wg, wu, wd, **expert)
    z_got = swap(both.reshape(16, 16, 256), "ep_0").reshape(256, 256)
    z_other, *act_other = call(expert_kernel, outs, other, wg, wu, wd, **expert)
    z_back = shift(z_other, "ep_2", 1)
    z_back, z_got = lax.optimization_barrier((z_back, z_got))
    dense_grad, share, dense_w = call(
        z_sum_kernel,
        (struct(8, 256, dtype=F32), struct(8, 128, dtype=F32), struct(128, 256)),
        z_got,
        gate_row,
        dense_t,
    )
    z_sum = call(add_kernel, outs[0], z_own, z_back)
    z_all = swap(z_sum, "tp")
    share = call(
        share_kernel, struct(8, 128, dtype=F32), share, shift(share, "ep_2", 1), after=(z_sum,)
    )
    shares = [share] + [shift(share, "tp", by) for by in (1, 2, 3)]
    back_ready = call(return_kernel, struct(512, 256), z_all, *shares)
    gate_grad, up_grad, down_grad, grads_done = call(
        grads_kernel,
        (struct(352, 1024),) * 3 + (struct(8, 128, dtype=F32),),
        own,
        other,
        *in_place(*act_own, *act_other),
        after=(back_ready,),
        scratch=(pltpu.VMEM((352, 1024), BF16),) * 3 + (pltpu.SemaphoreType.DMA((3,)),),
        out_specs=(hbm_spec,) * 3 + (vmem_spec,),
        flops=1_400_000_000,
    )
    back = swap(back_ready.reshape(64, 8, 256), CHIPS).reshape(512, 256)

    dense_w = lax.all_gather(dense_w, "ep_1", axis=0, tiled=True)
    dense_dx = call(
        dense_kernel,
        struct(128, 256, dtype=F32),
        cot_all,
        gate_row,
        dense_w,
        shift(dense_w, "ep_2", 1),
    )
    token_grad, route_t, mix_all = call(
        final_kernel,
        (struct(128, 256), struct(2, 128, dtype=F32), struct(EXPERTS, 128, dtype=F32)),
        back,
        keys,
        cols,
        dense_dx,
        after=(grads_done,),
    )
    mix_grad = mix_all[:, :16].reshape(1024)
    return (
        token_grad,
        route_t.T,
        gate_grad.T[None],
        up_grad.T[None],
        down_grad[None],
        dense_grad.T,
        mix_grad,
    )


def grads_kernel(
    own_ref, other_ref, dg0, du0, wt0, dg1, du1, wt1,
    gate_ref, up_ref, down_ref, done_ref, gate_tmp, up_tmp, down_tmp, sems,
):
    copies = []
    for n, (left0, left1, lo, out_ref, tmp) in enumerate((
        (dg0, dg1, 0, gate_ref, gate_tmp),
        (du0, du1, 0, up_ref, up_tmp),
        (wt0, wt1, 256, down_ref, down_tmp),
    )):
        left = jnp.concatenate([left0[...], left1[...]], axis=0)
        for t in range(TP):
            right = jnp.concatenate(
                [own_ref[t, 0:ROWS, lo : lo + 256], other_ref[t, 0:ROWS, lo : lo + 256]], axis=0
            )
            tmp[:, t * 256 : (t + 1) * 256] = dot_tn(left, right).astype(BF16)
        copies.append(pltpu.make_async_copy(tmp, out_ref, sems.at[n]))
        copies[-1].start()
    done_ref[...] = jnp.zeros((8, 128), F32)
    for copy in copies:
        copy.wait()


def solution(mesh):
    finer = Mesh(mesh.devices.reshape(16, 4, 2, mesh.shape["tp"]), ("ep_0", "ep_1", "ep_2", "tp"))
    in_specs = (
        P(EP, "tp"),
        P(EP, "tp"),
        P(EP, None),
        P(EP, None),
        P(EP, None, "tp"),
        P(EP, None, "tp"),
        P(EP, "tp", None),
        P("tp", EP),
        P(),
    )
    out_specs = (
        P(EP, "tp"),
        P(EP, None),
        P(EP, None, "tp"),
        P(EP, None, "tp"),
        P(EP, "tp", None),
        P("tp", EP),
        P(),
    )
    return jax.shard_map(local, mesh=finer, in_specs=in_specs, out_specs=out_specs, check_vma=False)
```

```python
import jax
import jax.numpy as jnp
from jax import lax
from jax.experimental import pallas as pl
from jax.experimental.pallas import tpu as pltpu
from jax.sharding import Mesh
from jax.sharding import PartitionSpec as P


EP = ("ep_0", "ep_1", "ep_2")
CHIPS = ("ep_0", "ep_1")
F32 = jnp.float32
BF16 = jnp.bfloat16
EXPERTS = 64
CAP = 5
ROWS = EXPERTS * CAP
EXTRA = 16
TP = 4


def iota(shape, dim):
    return lax.broadcasted_iota(jnp.int32, shape, dim)


def dot(a, b):
    return jnp.dot(a, b, preferred_element_type=F32)


def dot_nt(a, b):
    return lax.dot_general(a, b, (((1,), (1,)), ((), ())), preferred_element_type=F32)


def dot_tn(a, b):
    return lax.dot_general(a, b, (((0,), (0,)), ((), ())), preferred_element_type=F32)


def onehot(cond):
    return jnp.where(cond, 1.0, 0.0).astype(BF16)


def call(kernel, outs, *args, after=(), scratch=(), hbm=0, flops=0, out_specs=None):
    whole = pl.BlockSpec(memory_space=pltpu.VMEM)
    placed = pl.BlockSpec(memory_space=pl.ANY)
    in_hbm = pl.BlockSpec(memory_space=pltpu.HBM)
    count = len(args)

    def body(*refs):
        kernel(*refs[:count], *refs[count + len(after) :])

    return pl.pallas_call(
        body,
        out_shape=outs,
        in_specs=[in_hbm] * hbm + [whole] * (count - hbm) + [placed] * len(after),
        out_specs=out_specs or jax.tree.map(lambda _: whole, outs),
        scratch_shapes=list(scratch),
        cost_estimate=pl.CostEstimate(
            flops=flops or 200_000_000, bytes_accessed=1_000_000, transcendentals=0
        ),
        compiler_params=pltpu.CompilerParams(vmem_limit_bytes=20 * 1024 * 1024),
    )(*args, *after)


def struct(*shape, dtype=BF16):
    return jax.ShapeDtypeStruct(shape, dtype)


def pack_kernel(
    tok_hbm, cot_hbm, routes_ref, weights_ref, out_ref, keys_ref, cols_ref, cot_ref, tok_ref, sems
):
    tokens = 128
    tok_copy = pltpu.make_async_copy(tok_hbm, tok_ref, sems.at[0])
    cot_copy = pltpu.make_async_copy(cot_hbm, cot_ref, sems.at[1])
    tok_copy.start()
    cot_copy.start()
    r0 = routes_ref[0:1, :].astype(F32)
    r1 = routes_ref[1:2, :].astype(F32)
    w = weights_ref[...].astype(F32)
    row = iota((tokens, tokens), 0)
    lane = iota((tokens, tokens), 1)
    eye = row == lane

    def to_col(v):
        return jnp.sum(jnp.where(eye, v, 0.0), axis=1, keepdims=True)

    c0 = to_col(r0)
    c1 = to_col(r1)
    before = row < lane

    def rank_of(r):
        hit = jnp.where(c0 == r, 1.0, 0.0) + jnp.where(c1 == r, 1.0, 0.0)
        return jnp.sum(jnp.where(before, hit, 0.0), axis=0, keepdims=True)

    k0 = rank_of(r0)
    k1 = rank_of(r1)
    four = jnp.concatenate([(r0 * CAP + k0) * 4 + i for i in range(4)], axis=1)
    four_b = jnp.concatenate([(r1 * CAP + k1) * 4 + i for i in range(4)], axis=1)
    msgs = EXPERTS * 8
    m_row = iota((msgs, 512), 0)
    dest = m_row // 8
    sub = m_row % 8
    tok_copy.wait()
    cot_copy.wait()
    data = jnp.concatenate(
        [tok_ref[:, :128], tok_ref[:, 128:], cot_ref[:, :128], cot_ref[:, 128:]], axis=0
    )
    for j in range(3):
        cell = j * 8 + sub
        key = jnp.where(cell < 20, dest * 20 + cell, -1).astype(F32)
        block = dot(onehot((key == four) | (key == four_b)), data)
        if j == 2:
            both = jnp.concatenate([r0, r1], axis=1)
            there = onehot((m_row[:, :256].astype(F32) == both * 8 + 4))
            lane_f = lane.astype(F32)
            v0 = jnp.where(lane_f == to_col(k0), to_col(w[0:1, :]), 0.0)
            v1 = jnp.where(lane_f == to_col(k1), to_col(w[1:2, :]), 0.0)
            block = block + dot(there, jnp.concatenate([v0, v1], axis=0).astype(BF16))
        out_ref[:, j * 128 : (j + 1) * 128] = block.astype(BF16)
    eight = iota((8, tokens), 0)
    keys_ref[...] = jnp.where(
        eight == 0, r0, jnp.where(eight == 1, r1, jnp.where(eight == 2, k0, k1))
    )
    cols_ref[...] = jnp.where(
        lane == 0, to_col(r0 * 8 + k0), jnp.where(lane == 1, to_col(r1 * 8 + k1), 0.0)
    )


def unpack_kernel(in_ref, out_ref):
    msgs = EXPERTS * 8
    p_row = iota((512, msgs), 0)
    p_col = iota((512, msgs), 1)
    chunk = p_row // 128
    half = (p_row % 128) // 64
    src = p_row % 64
    perm = onehot(p_col == src * 8 + half * 4 + chunk)
    rows = dot(perm, in_ref[...])
    by_src = rows[64:128, 256:384]
    tall = jnp.concatenate([by_src] * CAP, axis=0)
    t_row = iota((ROWS, 128), 0)
    t_lane = iota((ROWS, 128), 1)
    tall = jnp.where(t_row // 64 == t_lane, tall, 0.0).astype(BF16)
    w_row = dot_nt(jnp.full((EXTRA, 128), 1.0, BF16), tall).astype(BF16)
    rows = rows.astype(BF16)
    for t in range(TP):
        for c in range(4):
            for j in range(3):
                n = 128 if j < 2 else 64
                out_ref[t, j * 128 : j * 128 + n, c * 128 : (c + 1) * 128] = rows[
                    c * 128 : c * 128 + n, j * 128 : (j + 1) * 128
                ]
        out_ref[t, ROWS : ROWS + EXTRA, :] = jnp.zeros((EXTRA, 512), BF16)
        out_ref[t, ROWS : ROWS + EXTRA, 0:ROWS] = w_row


def expert_kernel(
    in_ref, wg_ref, wu_ref, wd_ref, z_ref, dg_out, du_out, wt_out, dg_ref, du_ref, wt_ref, sems
):
    outward = [
        pltpu.make_async_copy(src, dst, sems.at[n])
        for n, (src, dst) in enumerate(((dg_ref, dg_out), (du_ref, du_out), (wt_ref, wt_out)))
    ]

    def summed(lo, w_ref):
        return sum(
            dot_nt(in_ref[t, 0:ROWS, lo : lo + 256], w_ref[:, t * 256 : (t + 1) * 256])
            for t in range(TP)
        )

    pre_gate = summed(0, wg_ref)
    pre_up = summed(0, wu_ref)
    projected = summed(256, wd_ref)
    w_row = in_ref[0, ROWS : ROWS + EXTRA, 0:ROWS].astype(F32)[0:1, :]
    eye = iota((ROWS, ROWS), 0) == iota((ROWS, ROWS), 1)
    weight = jnp.sum(jnp.where(eye, w_row, 0.0), axis=1, keepdims=True)
    sig = jax.nn.sigmoid(pre_gate)
    activated = pre_gate * sig
    hidden = activated * pre_up
    route = jnp.sum(hidden.astype(BF16).astype(F32) * projected, axis=1, keepdims=True)
    grad = weight * projected
    d_gate = (grad * pre_up * sig * (1.0 + pre_gate * (1.0 - sig))).astype(BF16)
    d_up = (grad * activated).astype(BF16)
    dg_ref[...] = d_gate
    du_ref[...] = d_up
    wt_ref[...] = (weight * hidden).astype(BF16)
    for copy in outward:
        copy.start()
    part = (dot(d_gate, wg_ref[...]) + dot(d_up, wu_ref[...])).astype(BF16)
    hi = route.astype(BF16).astype(F32)
    lo = route - hi
    lane = iota((ROWS, 128), 1)
    pair = jnp.where(lane == 0, hi, jnp.where(lane == 1, lo, 0.0))
    pair = jnp.concatenate([pair, jnp.zeros((512 - ROWS, 128), F32)], axis=0).astype(BF16)
    pick = onehot(iota((EXTRA, 128), 0) == iota((EXTRA, 128), 1))
    flat = dot_nt(pick, pair)
    extra = jnp.concatenate([flat[0:8, 0:256], flat[0:8, 256:512]], axis=0).astype(BF16)
    for t in range(TP):
        z_ref[t, 0:ROWS, :] = part[:, t * 256 : (t + 1) * 256]
        z_ref[t, ROWS : ROWS + EXTRA, :] = extra
    for copy in outward:
        copy.wait()


def load_kernel(*refs):
    count = (len(refs) - 1) // 2
    copies = [
        pltpu.make_async_copy(refs[n], refs[count + n], refs[-1].at[n]) for n in range(count)
    ]
    for copy in copies:
        copy.start()
    for copy in copies:
        copy.wait()


def return_kernel(in_ref, out_ref):
    total = sum(in_ref[t].astype(F32) for t in range(TP))
    msgs = EXPERTS * 8
    rows = total[0:ROWS].astype(BF16)
    m_row = iota((msgs, 512), 0)
    m_col = iota((msgs, 512), 1)
    dest = m_row // 8
    sub = m_row % 8
    perm = onehot((m_col == sub * 64 + dest) & (sub < CAP))
    out = dot(perm[:, 0:ROWS], rows)
    first = total[ROWS : ROWS + 1] + total[ROWS + 1 : ROWS + 2]
    second = total[ROWS + 8 : ROWS + 9] + total[ROWS + 9 : ROWS + 10]
    route = jnp.concatenate([first, second], axis=1)
    hi = route.astype(BF16).astype(F32)
    lo = route - hi
    mine = (sub == CAP) & (m_col % 64 == dest)
    b_row = iota((512, 256), 0)
    b_col = iota((512, 256), 1)
    out = out + dot(jnp.where(mine, hi, 0.0).astype(BF16), onehot(b_row // 64 == b_col))
    out = out + dot(jnp.where(mine, lo, 0.0).astype(BF16), onehot(b_row // 64 == b_col - 128))
    mix = total[ROWS + 2 : ROWS + 3, 0:128] + total[ROWS + 3 : ROWS + 4, 0:128]
    mix_hi = mix.astype(BF16).astype(F32)
    mix_row = jnp.concatenate([mix_hi, mix - mix_hi], axis=1)
    out_sub = iota((msgs, 256), 0) % 8
    out = jnp.where(out_sub == CAP + 1, mix_row, out)
    out_ref[...] = out.astype(BF16)


def final_kernel(in_ref, keys_ref, cols_ref, dense_ref, tok_ref, route_ref, mix_ref):
    msgs = EXPERTS * 8
    got = in_ref[...]
    lane = iota((128, msgs), 1).astype(F32)
    take = onehot((lane == cols_ref[:, 0:1]) | (lane == cols_ref[:, 1:2]))
    tok_ref[...] = (dot(take, got) + dense_ref[...]).astype(BF16)
    m_row = iota((msgs, 128), 0).astype(F32)
    l_row = iota((256, 128), 0).astype(F32)
    for a in range(2):
        expert = keys_ref[a : a + 1, :]
        rank = keys_ref[a + 2 : a + 3, :]
        cells = dot_tn(got, onehot(m_row == expert * 8 + CAP))
        keep = (l_row == rank) | (l_row == rank + 128)
        route_ref[a : a + 1, :] = jnp.sum(jnp.where(keep, cells, 0.0), axis=0, keepdims=True)
    e_row = iota((EXPERTS, msgs), 0)
    e_col = iota((EXPERTS, msgs), 1)
    mix = dot(onehot(e_col == e_row * 8 + CAP + 1), got)
    mix_ref[...] = mix[:, 0:128] + mix[:, 128:256]


def moment_kernel(cot_ref, tok_ref, keep_ref, send_ref):
    moment = dot_tn(cot_ref[...], tok_ref[...])
    north = lax.axis_index("ep_2") == 1
    for x in range(4):
        parts = []
        for c in range(2):
            starts = [(z * 8 + x * 2 + c) * 8 for z in range(16)]
            parts.append(jnp.concatenate([moment[s : s + 8] for s in starts], axis=0))
        span = slice(x * 128, (x + 1) * 128)
        keep_ref[span, :] = jnp.where(north, parts[1], parts[0])
        send_ref[span, :] = jnp.where(north, parts[0], parts[1]).astype(BF16)


def core_sum_kernel(keep_ref, got_ref, own_ref, s1_ref, s2_ref, s3_ref, sum_ref):
    sum_ref[...] = keep_ref[...] + got_ref[...].astype(F32)
    here = lax.axis_index("ep_1")

    def part(shift):
        start = pl.multiple_of(lax.rem(here + shift, 4) * 128, 128)
        return sum_ref[pl.ds(start, 128), :]

    own_ref[...] = part(0)
    s1_ref[...] = part(1).astype(BF16)
    s2_ref[...] = part(2).astype(BF16)
    s3_ref[...] = part(3).astype(BF16)


def x_sum_kernel(own_ref, r1_ref, r2_ref, r3_ref, dense_ref, out_ref):
    total = own_ref[...] + r1_ref[...].astype(F32)
    total = total + (r2_ref[...].astype(F32) + r3_ref[...].astype(F32))
    dense = dense_ref[...].astype(F32)
    pieces = []
    for z in range(16):
        pieces += [total[z * 8 : z * 8 + 8], dense]
    out_ref[...] = jnp.concatenate(pieces, axis=0).astype(BF16)


def z_sum_kernel(in_ref, gate_ref, dense_ref, grad_ref, share_ref, w_ref):
    got = in_ref[...].astype(F32)
    moment = sum(got[z * 16 : z * 16 + 8] for z in range(16)) * (1.0 / 128)
    w_ref[...] = jnp.concatenate(
        [got[z * 16 + 8 : z * 16 + 16] for z in range(16)], axis=0
    ).astype(BF16)
    core = lax.axis_index("ep_2")
    first = (lax.axis_index("ep_0") * 8 + lax.axis_index("ep_1") * 2 + core) * 8
    at = iota((8, 1024), 1) == first + iota((8, 1024), 0)
    gate = jnp.sum(jnp.where(at, gate_ref[...], 0.0), axis=1, keepdims=True)
    grad_ref[...] = moment * gate
    share = jnp.sum(moment * dense_ref[...].astype(F32), axis=1, keepdims=True)
    spot = iota((8, 128), 1) == core * 8 + iota((8, 128), 0)
    row = jnp.sum(jnp.where(spot, share, 0.0), axis=0, keepdims=True)
    share_ref[...] = jnp.broadcast_to(row, (8, 128))


def dense_kernel(cot_ref, gate_ref, own_ref, other_ref, out_ref):
    north = lax.axis_index("ep_2") == 1
    own = own_ref[...].astype(F32)
    other = other_ref[...].astype(F32)
    south_w = jnp.where(north, other, own)
    north_w = jnp.where(north, own, other)
    pieces = []
    for z in range(16):
        for x in range(4):
            s = (x * 16 + z) * 8
            pieces += [south_w[s : s + 8], north_w[s : s + 8]]
    weight = jnp.concatenate(pieces, axis=0).astype(BF16)
    scaled = (gate_ref[...] * cot_ref[...].astype(F32)).astype(BF16)
    out_ref[...] = dot(scaled, weight)


def add_kernel(a_ref, b_ref, m0_ref, m1_ref, out_ref):
    def parts(value):
        hi = value.astype(BF16).astype(F32)
        return hi, value - hi

    mix = parts(jnp.concatenate([m0_ref[0:1, :] + m1_ref[0:1, :], jnp.zeros((1, 128), F32)], axis=1))
    sub = iota((8, 256), 0)
    extra = []
    both = a_ref[0, ROWS : ROWS + EXTRA, :].astype(F32) + b_ref[0, ROWS : ROWS + EXTRA, :].astype(F32)
    for at in (0, 8):
        block = jnp.zeros((8, 256), F32)
        for n, row in enumerate(parts(both[at : at + 1] + both[at + 1 : at + 2]) + mix):
            block = jnp.where(sub == n, row, block)
        extra.append(block)
    extra = jnp.concatenate(extra, axis=0).astype(BF16)
    for t in range(TP):
        total = a_ref[t, 0:ROWS, :].astype(F32) + b_ref[t, 0:ROWS, :].astype(F32)
        out_ref[t, 0:ROWS, :] = total.astype(BF16)
        out_ref[t, ROWS : ROWS + EXTRA, :] = extra


def in_place(*arrays):
    return [pltpu.with_memory_space_constraint(a, pltpu.HBM) for a in arrays]


def swap(value, axes):
    return lax.all_to_all(value, axes, split_axis=0, concat_axis=0, tiled=True)


def shift(value, axis, by):
    n = lax.axis_size(axis)
    return lax.ppermute(value, axis, [(i, (i + by) % n) for i in range(n)])


def local(tokens, cotangent, routes, route_weights, w_gate, w_up, w_down, dense_weight, mix_gate):
    wg = w_gate[0].T
    wu = w_up[0].T
    wd = w_down[0]
    dense_t = dense_weight.T
    gate_row = mix_gate[None, :]
    tokens, cotangent, wg, wu, wd, routes_t, weights_t = in_place(
        tokens, cotangent, wg, wu, wd, routes.T, route_weights.T
    )
    packed, keys, cols, cot_here = call(
        pack_kernel,
        (
            struct(512, 384),
            struct(8, 128, dtype=F32),
            struct(128, 128, dtype=F32),
            struct(128, 256),
        ),
        tokens,
        cotangent,
        routes_t,
        weights_t,
        hbm=2,
        scratch=(
            pltpu.VMEM((128, 256), BF16),
            pltpu.SemaphoreType.DMA((2,)),
        ),
    )
    arrived = swap(packed.reshape(64, 8, 384), CHIPS)

    cot_all = lax.all_gather(cot_here, "tp", axis=1, tiled=True)
    keep, send = call(
        moment_kernel, (struct(512, 256, dtype=F32), struct(512, 256)), cot_all, tokens
    )
    here, *away = call(
        core_sum_kernel,
        (struct(128, 256, dtype=F32),) + (struct(128, 256),) * 3,
        keep,
        shift(send, "ep_2", 1),
        scratch=(pltpu.VMEM((512, 256), F32),),
    )
    both = call(
        x_sum_kernel,
        struct(256, 256),
        here,
        *(shift(piece, "ep_1", i + 1) for i, piece in enumerate(away)),
        dense_t,
    )

    own = call(
        unpack_kernel, struct(TP, ROWS + EXTRA, 512), arrived.reshape(512, 384), after=(here,)
    )
    own, both = lax.optimization_barrier((swap(own, "tp"), both))
    other = shift(own, "ep_2", 1)
    outs = (struct(TP, ROWS + EXTRA, 256),) + (pltpu.HBM((ROWS, 352), BF16),) * 3
    hbm_spec = pl.BlockSpec(memory_space=pltpu.HBM)
    vmem_spec = pl.BlockSpec(memory_space=pltpu.VMEM)
    expert = dict(
        flops=1_150_000_000,
        out_specs=(vmem_spec,) + (hbm_spec,) * 3,
        scratch=(pltpu.VMEM((ROWS, 352), BF16),) * 3 + (pltpu.SemaphoreType.DMA((3,)),),
    )
    weights = call(
        load_kernel,
        (struct(352, 1024),) * 3,
        wg,
        wu,
        wd,
        hbm=3,
        scratch=(pltpu.SemaphoreType.DMA((3,)),),
    )
    z_own, *act_own = call(expert_kernel, outs, own, *weights, **expert)
    z_got = swap(both.reshape(16, 16, 256), "ep_0").reshape(256, 256)
    z_other, *act_other = call(expert_kernel, outs, other, *weights, **expert)
    z_back = shift(z_other, "ep_2", 1)
    z_back, z_got = lax.optimization_barrier((z_back, z_got))
    dense_grad, share, dense_w = call(
        z_sum_kernel,
        (struct(8, 256, dtype=F32), struct(8, 128, dtype=F32), struct(128, 256)),
        z_got,
        gate_row,
        dense_t,
    )
    z_sum = call(add_kernel, outs[0], z_own, z_back, share, shift(share, "ep_2", 1))
    z_all = swap(z_sum, "tp")
    dense_w = lax.all_gather(dense_w, "ep_1", axis=0, tiled=True)
    z_all, dense_w = lax.optimization_barrier((z_all, dense_w))
    back_ready = call(return_kernel, struct(512, 256), z_all)
    gate_grad, up_grad, down_grad, grads_done = call(
        grads_kernel,
        (struct(352, 1024),) * 3 + (struct(8, 128, dtype=F32),),
        own,
        other,
        *in_place(*act_own, *act_other),
        after=(back_ready,),
        scratch=(pltpu.VMEM((352, 1024), BF16),) * 3 + (pltpu.SemaphoreType.DMA((3,)),),
        out_specs=(hbm_spec,) * 3 + (vmem_spec,),
        flops=1_400_000_000,
    )
    back = swap(back_ready.reshape(64, 8, 256), CHIPS).reshape(512, 256)

    dense_dx = call(
        dense_kernel,
        struct(128, 256, dtype=F32),
        cot_all,
        gate_row,
        dense_w,
        shift(dense_w, "ep_2", 1),
    )
    token_grad, route_t, mix_all = call(
        final_kernel,
        (struct(128, 256), struct(2, 128, dtype=F32), struct(EXPERTS, 128, dtype=F32)),
        back,
        keys,
        cols,
        dense_dx,
        after=(grads_done,),
    )
    mix_grad = mix_all[:, :16].reshape(1024)
    return (
        token_grad,
        route_t.T,
        gate_grad.T[None],
        up_grad.T[None],
        down_grad[None],
        dense_grad.T,
        mix_grad,
    )


def grads_kernel(
    own_ref, other_ref, dg0, du0, wt0, dg1, du1, wt1,
    gate_ref, up_ref, down_ref, done_ref, gate_tmp, up_tmp, down_tmp, sems,
):
    copies = []
    for n, (left0, left1, lo, out_ref, tmp) in enumerate((
        (dg0, dg1, 0, gate_ref, gate_tmp),
        (du0, du1, 0, up_ref, up_tmp),
        (wt0, wt1, 256, down_ref, down_tmp),
    )):
        left = jnp.concatenate([left0[...], left1[...]], axis=0)
        for t in range(TP):
            right = jnp.concatenate(
                [own_ref[t, 0:ROWS, lo : lo + 256], other_ref[t, 0:ROWS, lo : lo + 256]], axis=0
            )
            tmp[:, t * 256 : (t + 1) * 256] = dot_tn(left, right).astype(BF16)
        copies.append(pltpu.make_async_copy(tmp, out_ref, sems.at[n]))
        copies[-1].start()
    done_ref[...] = jnp.zeros((8, 128), F32)
    for copy in copies:
        copy.wait()


def solution(mesh):
    finer = Mesh(mesh.devices.reshape(16, 4, 2, mesh.shape["tp"]), ("ep_0", "ep_1", "ep_2", "tp"))
    in_specs = (
        P(EP, "tp"),
        P(EP, "tp"),
        P(EP, None),
        P(EP, None),
        P(EP, None, "tp"),
        P(EP, None, "tp"),
        P(EP, "tp", None),
        P("tp", EP),
        P(),
    )
    out_specs = (
        P(EP, "tp"),
        P(EP, None),
        P(EP, None, "tp"),
        P(EP, None, "tp"),
        P(EP, "tp", None),
        P("tp", EP),
        P(),
    )
    return jax.shard_map(local, mesh=finer, in_specs=in_specs, out_specs=out_specs, check_vma=False)
```

```python
import jax
import jax.numpy as jnp
from jax import lax
from jax.experimental import pallas as pl
from jax.experimental.pallas import tpu as pltpu
from jax.sharding import Mesh
from jax.sharding import PartitionSpec as P


EP = ("ep_0", "ep_1", "ep_2")
CHIPS = ("ep_1", "ep_0")
F32 = jnp.float32
BF16 = jnp.bfloat16
EXPERTS = 64
CAP = 5
ROWS = EXPERTS * CAP
EXTRA = 16
TP = 4


def iota(shape, dim):
    return lax.broadcasted_iota(jnp.int32, shape, dim)


def dot(a, b):
    return jnp.dot(a, b, preferred_element_type=F32)


def dot_nt(a, b):
    return lax.dot_general(a, b, (((1,), (1,)), ((), ())), preferred_element_type=F32)


def dot_tn(a, b):
    return lax.dot_general(a, b, (((0,), (0,)), ((), ())), preferred_element_type=F32)


def onehot(cond):
    return jnp.where(cond, 1.0, 0.0).astype(BF16)


def call(kernel, outs, *args, after=(), scratch=(), hbm=0, flops=0, out_specs=None):
    whole = pl.BlockSpec(memory_space=pltpu.VMEM)
    placed = pl.BlockSpec(memory_space=pl.ANY)
    in_hbm = pl.BlockSpec(memory_space=pltpu.HBM)
    count = len(args)

    def body(*refs):
        kernel(*refs[:count], *refs[count + len(after) :])

    return pl.pallas_call(
        body,
        out_shape=outs,
        in_specs=[in_hbm] * hbm + [whole] * (count - hbm) + [placed] * len(after),
        out_specs=out_specs or jax.tree.map(lambda _: whole, outs),
        scratch_shapes=list(scratch),
        cost_estimate=pl.CostEstimate(
            flops=flops or 200_000_000, bytes_accessed=1_000_000, transcendentals=0
        ),
        compiler_params=pltpu.CompilerParams(vmem_limit_bytes=20 * 1024 * 1024),
    )(*args, *after)


def struct(*shape, dtype=BF16):
    return jax.ShapeDtypeStruct(shape, dtype)


def peer_of(expert):
    return (expert & 3) * 16 + (expert >> 2)


def pack_kernel(
    tok_ref, cot_ref, routes_ref, weights_ref, out_ref, keys_ref, cols_ref, cot_out
):
    tokens = 128
    cot_out[...] = cot_ref[...]
    r0 = peer_of(routes_ref[0:1, :]).astype(F32)
    r1 = peer_of(routes_ref[1:2, :]).astype(F32)
    w = weights_ref[...].astype(F32)
    row = iota((tokens, tokens), 0)
    lane = iota((tokens, tokens), 1)
    eye = row == lane

    def to_col(v):
        return jnp.sum(jnp.where(eye, v, 0.0), axis=1, keepdims=True)

    c0 = to_col(r0)
    c1 = to_col(r1)
    before = row < lane

    def rank_of(r):
        hit = jnp.where(c0 == r, 1.0, 0.0) + jnp.where(c1 == r, 1.0, 0.0)
        return jnp.sum(jnp.where(before, hit, 0.0), axis=0, keepdims=True)

    k0 = rank_of(r0)
    k1 = rank_of(r1)
    four = jnp.concatenate([(r0 * CAP + k0) * 4 + i for i in range(4)], axis=1)
    four_b = jnp.concatenate([(r1 * CAP + k1) * 4 + i for i in range(4)], axis=1)
    msgs = EXPERTS * 8
    m_row = iota((msgs, 512), 0)
    dest = m_row // 8
    sub = m_row % 8
    data = jnp.concatenate(
        [tok_ref[:, :128], tok_ref[:, 128:], cot_ref[:, :128], cot_ref[:, 128:]], axis=0
    )
    for j in range(3):
        cell = j * 8 + sub
        key = jnp.where(cell < 20, dest * 20 + cell, -1).astype(F32)
        block = dot(onehot((key == four) | (key == four_b)), data)
        if j == 2:
            both = jnp.concatenate([r0, r1], axis=1)
            there = onehot((m_row[:, :256].astype(F32) == both * 8 + 4))
            lane_f = lane.astype(F32)
            v0 = jnp.where(lane_f == to_col(k0), to_col(w[0:1, :]), 0.0)
            v1 = jnp.where(lane_f == to_col(k1), to_col(w[1:2, :]), 0.0)
            block = block + dot(there, jnp.concatenate([v0, v1], axis=0).astype(BF16))
        out_ref[:, j * 128 : (j + 1) * 128] = block.astype(BF16)
    eight = iota((8, tokens), 0)
    keys_ref[...] = jnp.where(
        eight == 0, r0, jnp.where(eight == 1, r1, jnp.where(eight == 2, k0, k1))
    )
    cols_ref[...] = jnp.where(
        lane == 0, to_col(r0 * 8 + k0), jnp.where(lane == 1, to_col(r1 * 8 + k1), 0.0)
    )


def unpack_kernel(in_ref, out_ref):
    msgs = EXPERTS * 8
    p_row = iota((512, msgs), 0)
    p_col = iota((512, msgs), 1)
    chunk = p_row // 128
    half = (p_row % 128) // 64
    src = p_row % 64
    perm = onehot(p_col == src * 8 + half * 4 + chunk)
    rows = dot(perm, in_ref[...])
    by_src = rows[64:128, 256:384]
    tall = jnp.concatenate([by_src] * CAP, axis=0)
    t_row = iota((ROWS, 128), 0)
    t_lane = iota((ROWS, 128), 1)
    tall = jnp.where(t_row // 64 == t_lane, tall, 0.0).astype(BF16)
    w_row = dot_nt(jnp.full((EXTRA, 128), 1.0, BF16), tall).astype(BF16)
    rows = rows.astype(BF16)
    for t in range(TP):
        for c in range(4):
            for j in range(3):
                n = 128 if j < 2 else 64
                out_ref[t, j * 128 : j * 128 + n, c * 128 : (c + 1) * 128] = rows[
                    c * 128 : c * 128 + n, j * 128 : (j + 1) * 128
                ]
        out_ref[t, ROWS : ROWS + EXTRA, :] = jnp.zeros((EXTRA, 512), BF16)
        out_ref[t, ROWS : ROWS + EXTRA, 0:ROWS] = w_row


def expert_kernel(
    in_ref, wg_ref, wu_ref, wd_ref, z_ref, dg_out, du_out, wt_out, dg_ref, du_ref, wt_ref, sems
):
    outward = [
        pltpu.make_async_copy(src, dst, sems.at[n])
        for n, (src, dst) in enumerate(((dg_ref, dg_out), (du_ref, du_out), (wt_ref, wt_out)))
    ]

    def summed(lo, w_ref):
        return sum(
            dot_nt(in_ref[t, 0:ROWS, lo : lo + 256], w_ref[:, t * 256 : (t + 1) * 256])
            for t in range(TP)
        )

    pre_gate = summed(0, wg_ref)
    pre_up = summed(0, wu_ref)
    projected = summed(256, wd_ref)
    w_row = in_ref[0, ROWS : ROWS + EXTRA, 0:ROWS].astype(F32)[0:1, :]
    eye = iota((ROWS, ROWS), 0) == iota((ROWS, ROWS), 1)
    weight = jnp.sum(jnp.where(eye, w_row, 0.0), axis=1, keepdims=True)
    sig = jax.nn.sigmoid(pre_gate)
    activated = pre_gate * sig
    hidden = activated * pre_up
    route = jnp.sum(hidden.astype(BF16).astype(F32) * projected, axis=1, keepdims=True)
    grad = weight * projected
    d_gate = (grad * pre_up * sig * (1.0 + pre_gate * (1.0 - sig))).astype(BF16)
    d_up = (grad * activated).astype(BF16)
    dg_ref[...] = d_gate
    du_ref[...] = d_up
    wt_ref[...] = (weight * hidden).astype(BF16)
    for copy in outward:
        copy.start()
    part = (dot(d_gate, wg_ref[...]) + dot(d_up, wu_ref[...])).astype(BF16)
    hi = route.astype(BF16).astype(F32)
    lo = route - hi
    lane = iota((ROWS, 128), 1)
    pair = jnp.where(lane == 0, hi, jnp.where(lane == 1, lo, 0.0))
    pair = jnp.concatenate([pair, jnp.zeros((512 - ROWS, 128), F32)], axis=0).astype(BF16)
    pick = onehot(iota((EXTRA, 128), 0) == iota((EXTRA, 128), 1))
    flat = dot_nt(pick, pair)
    extra = jnp.concatenate([flat[0:8, 0:256], flat[0:8, 256:512]], axis=0).astype(BF16)
    for t in range(TP):
        z_ref[t, 0:ROWS, :] = part[:, t * 256 : (t + 1) * 256]
        z_ref[t, ROWS : ROWS + EXTRA, :] = extra
    for copy in outward:
        copy.wait()


def load_kernel(*refs):
    count = (len(refs) - 1) // 2
    copies = [
        pltpu.make_async_copy(refs[n], refs[count + n], refs[-1].at[n]) for n in range(count)
    ]
    for copy in copies:
        copy.start()
    for copy in copies:
        copy.wait()


def return_kernel(in_ref, out_ref):
    total = sum(in_ref[t].astype(F32) for t in range(TP))
    msgs = EXPERTS * 8
    rows = total[0:ROWS].astype(BF16)
    m_row = iota((msgs, 512), 0)
    m_col = iota((msgs, 512), 1)
    dest = m_row // 8
    sub = m_row % 8
    perm = onehot((m_col == sub * 64 + dest) & (sub < CAP))
    out = dot(perm[:, 0:ROWS], rows)
    first = total[ROWS : ROWS + 1] + total[ROWS + 1 : ROWS + 2]
    second = total[ROWS + 8 : ROWS + 9] + total[ROWS + 9 : ROWS + 10]
    route = jnp.concatenate([first, second], axis=1)
    hi = route.astype(BF16).astype(F32)
    lo = route - hi
    mine = (sub == CAP) & (m_col % 64 == dest)
    b_row = iota((512, 256), 0)
    b_col = iota((512, 256), 1)
    out = out + dot(jnp.where(mine, hi, 0.0).astype(BF16), onehot(b_row // 64 == b_col))
    out = out + dot(jnp.where(mine, lo, 0.0).astype(BF16), onehot(b_row // 64 == b_col - 128))
    mix = total[ROWS + 2 : ROWS + 3, 0:128] + total[ROWS + 3 : ROWS + 4, 0:128]
    mix_hi = mix.astype(BF16).astype(F32)
    mix_row = jnp.concatenate([mix_hi, mix - mix_hi], axis=1)
    out_sub = iota((msgs, 256), 0) % 8
    out = jnp.where(out_sub == CAP + 1, mix_row, out)
    out_ref[...] = out.astype(BF16)


def final_kernel(in_ref, keys_ref, cols_ref, dense_ref, tok_ref, route_ref, mix_ref):
    msgs = EXPERTS * 8
    got = in_ref[...]
    lane = iota((128, msgs), 1).astype(F32)
    take = onehot((lane == cols_ref[:, 0:1]) | (lane == cols_ref[:, 1:2]))
    tok_ref[...] = (dot(take, got) + dense_ref[...]).astype(BF16)
    m_row = iota((msgs, 128), 0).astype(F32)
    l_row = iota((256, 128), 0).astype(F32)
    for a in range(2):
        expert = keys_ref[a : a + 1, :]
        rank = keys_ref[a + 2 : a + 3, :]
        cells = dot_tn(got, onehot(m_row == expert * 8 + CAP))
        keep = (l_row == rank) | (l_row == rank + 128)
        route_ref[a : a + 1, :] = jnp.sum(jnp.where(keep, cells, 0.0), axis=0, keepdims=True)
    e_row = iota((EXPERTS, msgs), 0)
    e_col = iota((EXPERTS, msgs), 1)
    mix = dot(onehot(e_col == peer_of(e_row) * 8 + CAP + 1), got)
    mix_ref[...] = mix[:, 0:128] + mix[:, 128:256]


def moment_kernel(cot_ref, tok_ref, keep_ref, send_ref):
    moment = dot_tn(cot_ref[...], tok_ref[...])
    north = lax.axis_index("ep_2") == 1
    for x in range(4):
        parts = []
        for c in range(2):
            starts = [(z * 8 + x * 2 + c) * 8 for z in range(16)]
            parts.append(jnp.concatenate([moment[s : s + 8] for s in starts], axis=0))
        span = slice(x * 128, (x + 1) * 128)
        keep_ref[span, :] = jnp.where(north, parts[1], parts[0])
        send_ref[span, :] = jnp.where(north, parts[0], parts[1]).astype(BF16)


def core_sum_kernel(keep_ref, got_ref, own_ref, s1_ref, s2_ref, s3_ref, sum_ref):
    sum_ref[...] = keep_ref[...] + got_ref[...].astype(F32)
    here = lax.axis_index("ep_1")

    def part(shift):
        start = pl.multiple_of(lax.rem(here + shift, 4) * 128, 128)
        return sum_ref[pl.ds(start, 128), :]

    own_ref[...] = part(0)
    s1_ref[...] = part(1).astype(BF16)
    s2_ref[...] = part(2).astype(BF16)
    s3_ref[...] = part(3).astype(BF16)


def x_sum_kernel(own_ref, r1_ref, r2_ref, r3_ref, dense_ref, out_ref):
    total = own_ref[...] + r1_ref[...].astype(F32)
    total = total + (r2_ref[...].astype(F32) + r3_ref[...].astype(F32))
    dense = dense_ref[...].astype(F32)
    pieces = []
    for z in range(16):
        pieces += [total[z * 8 : z * 8 + 8], dense]
    out_ref[...] = jnp.concatenate(pieces, axis=0).astype(BF16)


def z_sum_kernel(in_ref, gate_ref, dense_ref, grad_ref, share_ref, w_ref):
    got = in_ref[...].astype(F32)
    moment = sum(got[z * 16 : z * 16 + 8] for z in range(16)) * (1.0 / 128)
    w_ref[...] = jnp.concatenate(
        [got[z * 16 + 8 : z * 16 + 16] for z in range(16)], axis=0
    ).astype(BF16)
    core = lax.axis_index("ep_2")
    first = (lax.axis_index("ep_0") * 8 + lax.axis_index("ep_1") * 2 + core) * 8
    at = iota((8, 1024), 1) == first + iota((8, 1024), 0)
    gate = jnp.sum(jnp.where(at, gate_ref[...], 0.0), axis=1, keepdims=True)
    grad_ref[...] = moment * gate
    share = jnp.sum(moment * dense_ref[...].astype(F32), axis=1, keepdims=True)
    spot = iota((8, 128), 1) == core * 8 + iota((8, 128), 0)
    row = jnp.sum(jnp.where(spot, share, 0.0), axis=0, keepdims=True)
    share_ref[...] = jnp.broadcast_to(row, (8, 128))


def dense_kernel(cot_ref, gate_ref, own_ref, other_ref, out_ref):
    north = lax.axis_index("ep_2") == 1
    own = own_ref[...].astype(F32)
    other = other_ref[...].astype(F32)
    south_w = jnp.where(north, other, own)
    north_w = jnp.where(north, own, other)
    pieces = []
    for z in range(16):
        for x in range(4):
            s = (x * 16 + z) * 8
            pieces += [south_w[s : s + 8], north_w[s : s + 8]]
    weight = jnp.concatenate(pieces, axis=0).astype(BF16)
    scaled = (gate_ref[...] * cot_ref[...].astype(F32)).astype(BF16)
    out_ref[...] = dot(scaled, weight)


def add_kernel(a_ref, b_ref, m0_ref, m1_ref, out_ref):
    def parts(value):
        hi = value.astype(BF16).astype(F32)
        return hi, value - hi

    mix = parts(jnp.concatenate([m0_ref[0:1, :] + m1_ref[0:1, :], jnp.zeros((1, 128), F32)], axis=1))
    sub = iota((8, 256), 0)
    extra = []
    both = a_ref[0, ROWS : ROWS + EXTRA, :].astype(F32) + b_ref[0, ROWS : ROWS + EXTRA, :].astype(F32)
    for at in (0, 8):
        block = jnp.zeros((8, 256), F32)
        for n, row in enumerate(parts(both[at : at + 1] + both[at + 1 : at + 2]) + mix):
            block = jnp.where(sub == n, row, block)
        extra.append(block)
    extra = jnp.concatenate(extra, axis=0).astype(BF16)
    for t in range(TP):
        total = a_ref[t, 0:ROWS, :].astype(F32) + b_ref[t, 0:ROWS, :].astype(F32)
        out_ref[t, 0:ROWS, :] = total.astype(BF16)
        out_ref[t, ROWS : ROWS + EXTRA, :] = extra


def in_place(*arrays):
    return [pltpu.with_memory_space_constraint(a, pltpu.HBM) for a in arrays]


def swap(value, axes):
    return lax.all_to_all(value, axes, split_axis=0, concat_axis=0, tiled=True)


def shift(value, axis, by):
    n = lax.axis_size(axis)
    return lax.ppermute(value, axis, [(i, (i + by) % n) for i in range(n)])


def local(tokens, cotangent, routes, route_weights, w_gate, w_up, w_down, dense_weight, mix_gate):
    wg = w_gate[0].T
    wu = w_up[0].T
    wd = w_down[0]
    dense_t = dense_weight.T
    gate_row = mix_gate[None, :]
    tokens, cotangent, wg, wu, wd, routes_t, weights_t = in_place(
        tokens, cotangent, wg, wu, wd, routes.T, route_weights.T
    )
    packed, keys, cols, cot_here = call(
        pack_kernel,
        (
            struct(512, 384),
            struct(8, 128, dtype=F32),
            struct(128, 128, dtype=F32),
            struct(128, 256),
        ),
        tokens,
        cotangent,
        routes_t,
        weights_t,
    )
    arrived = swap(packed.reshape(64, 8, 384), CHIPS)

    cot_all = lax.all_gather(cot_here, "tp", axis=1, tiled=True)
    keep, send = call(
        moment_kernel, (struct(512, 256, dtype=F32), struct(512, 256)), cot_all, tokens
    )
    here, *away = call(
        core_sum_kernel,
        (struct(128, 256, dtype=F32),) + (struct(128, 256),) * 3,
        keep,
        shift(send, "ep_2", 1),
        scratch=(pltpu.VMEM((512, 256), F32),),
    )
    both = call(
        x_sum_kernel,
        struct(256, 256),
        here,
        *(shift(piece, "ep_1", i + 1) for i, piece in enumerate(away)),
        dense_t,
    )

    own = call(
        unpack_kernel, struct(TP, ROWS + EXTRA, 512), arrived.reshape(512, 384), after=(here,)
    )
    own, both = lax.optimization_barrier((swap(own, "tp"), both))
    other = shift(own, "ep_2", 1)
    outs = (struct(TP, ROWS + EXTRA, 256),) + (pltpu.HBM((ROWS, 352), BF16),) * 3
    hbm_spec = pl.BlockSpec(memory_space=pltpu.HBM)
    vmem_spec = pl.BlockSpec(memory_space=pltpu.VMEM)
    expert = dict(
        flops=1_150_000_000,
        out_specs=(vmem_spec,) + (hbm_spec,) * 3,
        scratch=(pltpu.VMEM((ROWS, 352), BF16),) * 3 + (pltpu.SemaphoreType.DMA((3,)),),
    )
    weights = call(
        load_kernel,
        (struct(352, 1024),) * 3,
        wg,
        wu,
        wd,
        hbm=3,
        scratch=(pltpu.SemaphoreType.DMA((3,)),),
    )
    z_own, *act_own = call(expert_kernel, outs, own, *weights, **expert)
    z_got = swap(both.reshape(16, 16, 256), "ep_0").reshape(256, 256)
    z_other, *act_other = call(expert_kernel, outs, other, *weights, **expert)
    z_back = shift(z_other, "ep_2", 1)
    z_back, z_got = lax.optimization_barrier((z_back, z_got))
    dense_grad, share, dense_w = call(
        z_sum_kernel,
        (struct(8, 256, dtype=F32), struct(8, 128, dtype=F32), struct(128, 256)),
        z_got,
        gate_row,
        dense_t,
    )
    z_sum = call(add_kernel, outs[0], z_own, z_back, share, shift(share, "ep_2", 1))
    z_all = swap(z_sum, "tp")
    dense_w = lax.all_gather(dense_w, "ep_1", axis=0, tiled=True)
    z_all, dense_w = lax.optimization_barrier((z_all, dense_w))
    back_ready = call(return_kernel, struct(512, 256), z_all)
    gate_grad, up_grad, down_grad, grads_done = call(
        grads_kernel,
        (struct(352, 1024),) * 3 + (struct(8, 128, dtype=F32),),
        own,
        other,
        *in_place(*act_own, *act_other),
        after=(back_ready,),
        scratch=(pltpu.VMEM((352, 1024), BF16),) * 3 + (pltpu.SemaphoreType.DMA((3,)),),
        out_specs=(hbm_spec,) * 3 + (vmem_spec,),
        flops=1_400_000_000,
    )
    back = swap(back_ready.reshape(64, 8, 256), CHIPS).reshape(512, 256)

    dense_dx = call(
        dense_kernel,
        struct(128, 256, dtype=F32),
        cot_all,
        gate_row,
        dense_w,
        shift(dense_w, "ep_2", 1),
    )
    token_grad, route_t, mix_all = call(
        final_kernel,
        (struct(128, 256), struct(2, 128, dtype=F32), struct(EXPERTS, 128, dtype=F32)),
        back,
        keys,
        cols,
        dense_dx,
        after=(grads_done,),
    )
    mix_grad = mix_all[:, :16].reshape(1024)
    return (
        token_grad,
        route_t.T,
        gate_grad.T[None],
        up_grad.T[None],
        down_grad[None],
        dense_grad.T,
        mix_grad,
    )


def grads_kernel(
    own_ref, other_ref, dg0, du0, wt0, dg1, du1, wt1,
    gate_ref, up_ref, down_ref, done_ref, gate_tmp, up_tmp, down_tmp, sems,
):
    copies = []
    for n, (left0, left1, lo, out_ref, tmp) in enumerate((
        (dg0, dg1, 0, gate_ref, gate_tmp),
        (du0, du1, 0, up_ref, up_tmp),
        (wt0, wt1, 256, down_ref, down_tmp),
    )):
        left = jnp.concatenate([left0[...], left1[...]], axis=0)
        for t in range(TP):
            right = jnp.concatenate(
                [own_ref[t, 0:ROWS, lo : lo + 256], other_ref[t, 0:ROWS, lo : lo + 256]], axis=0
            )
            tmp[:, t * 256 : (t + 1) * 256] = dot_tn(left, right).astype(BF16)
        copies.append(pltpu.make_async_copy(tmp, out_ref, sems.at[n]))
        copies[-1].start()
    done_ref[...] = jnp.zeros((8, 128), F32)
    for copy in copies:
        copy.wait()


def solution(mesh):
    finer = Mesh(mesh.devices.reshape(16, 4, 2, mesh.shape["tp"]), ("ep_0", "ep_1", "ep_2", "tp"))
    in_specs = (
        P(EP, "tp"),
        P(EP, "tp"),
        P(EP, None),
        P(EP, None),
        P(EP, None, "tp"),
        P(EP, None, "tp"),
        P(EP, "tp", None),
        P("tp", EP),
        P(),
    )
    out_specs = (
        P(EP, "tp"),
        P(EP, None),
        P(EP, None, "tp"),
        P(EP, None, "tp"),
        P(EP, "tp", None),
        P("tp", EP),
        P(),
    )
    return jax.shard_map(local, mesh=finer, in_specs=in_specs, out_specs=out_specs, check_vma=False)
```

```python
import jax
import jax.numpy as jnp
from jax import lax
from jax.experimental import pallas as pl
from jax.experimental.pallas import tpu as pltpu
from jax.sharding import Mesh
from jax.sharding import PartitionSpec as P


EP = ("ep_0", "ep_1", "ep_2")
CHIPS = ("ep_1", "ep_0")
F32 = jnp.float32
BF16 = jnp.bfloat16
EXPERTS = 64
CAP = 5
ROWS = EXPERTS * CAP
EXTRA = 16
TP = 4


def iota(shape, dim):
    return lax.broadcasted_iota(jnp.int32, shape, dim)


def dot(a, b):
    return jnp.dot(a, b, preferred_element_type=F32)


def dot_nt(a, b):
    return lax.dot_general(a, b, (((1,), (1,)), ((), ())), preferred_element_type=F32)


def dot_tn(a, b):
    return lax.dot_general(a, b, (((0,), (0,)), ((), ())), preferred_element_type=F32)


def onehot(cond):
    return jnp.where(cond, 1.0, 0.0).astype(BF16)


def call(kernel, outs, *args, after=(), scratch=(), hbm=0, flops=0, out_specs=None):
    whole = pl.BlockSpec(memory_space=pltpu.VMEM)
    placed = pl.BlockSpec(memory_space=pl.ANY)
    in_hbm = pl.BlockSpec(memory_space=pltpu.HBM)
    count = len(args)

    def body(*refs):
        kernel(*refs[:count], *refs[count + len(after) :])

    return pl.pallas_call(
        body,
        out_shape=outs,
        in_specs=[in_hbm] * hbm + [whole] * (count - hbm) + [placed] * len(after),
        out_specs=out_specs or jax.tree.map(lambda _: whole, outs),
        scratch_shapes=list(scratch),
        cost_estimate=pl.CostEstimate(
            flops=flops or 200_000_000, bytes_accessed=1_000_000, transcendentals=0
        ),
        compiler_params=pltpu.CompilerParams(vmem_limit_bytes=20 * 1024 * 1024),
    )(*args, *after)


def struct(*shape, dtype=BF16):
    return jax.ShapeDtypeStruct(shape, dtype)


def peer_of(expert):
    return (expert & 3) * 16 + (expert >> 2)


def pack_kernel(
    tok_ref, cot_ref, routes_ref, weights_ref, out_ref, keys_ref, cols_ref, cot_out
):
    tokens = 128
    cot_out[...] = cot_ref[...]
    r0 = peer_of(routes_ref[0:1, :]).astype(F32)
    r1 = peer_of(routes_ref[1:2, :]).astype(F32)
    w = weights_ref[...].astype(F32)
    row = iota((tokens, tokens), 0)
    lane = iota((tokens, tokens), 1)
    eye = row == lane

    def to_col(v):
        return jnp.sum(jnp.where(eye, v, 0.0), axis=1, keepdims=True)

    c0 = to_col(r0)
    c1 = to_col(r1)
    before = row < lane

    def rank_of(r):
        hit = jnp.where(c0 == r, 1.0, 0.0) + jnp.where(c1 == r, 1.0, 0.0)
        return jnp.sum(jnp.where(before, hit, 0.0), axis=0, keepdims=True)

    k0 = rank_of(r0)
    k1 = rank_of(r1)
    four = jnp.concatenate([(r0 * CAP + k0) * 4 + i for i in range(4)], axis=1)
    four_b = jnp.concatenate([(r1 * CAP + k1) * 4 + i for i in range(4)], axis=1)
    msgs = EXPERTS * 8
    m_row = iota((msgs, 512), 0)
    dest = m_row // 8
    sub = m_row % 8
    data = jnp.concatenate(
        [tok_ref[:, :128], tok_ref[:, 128:], cot_ref[:, :128], cot_ref[:, 128:]], axis=0
    )
    for j in range(3):
        cell = j * 8 + sub
        key = jnp.where(cell < 20, dest * 20 + cell, -1).astype(F32)
        block = dot(onehot((key == four) | (key == four_b)), data)
        if j == 2:
            both = jnp.concatenate([r0, r1], axis=1)
            there = onehot((m_row[:, :256].astype(F32) == both * 8 + 4))
            lane_f = lane.astype(F32)
            v0 = jnp.where(lane_f == to_col(k0), to_col(w[0:1, :]), 0.0)
            v1 = jnp.where(lane_f == to_col(k1), to_col(w[1:2, :]), 0.0)
            block = block + dot(there, jnp.concatenate([v0, v1], axis=0).astype(BF16))
        out_ref[:, j * 128 : (j + 1) * 128] = block.astype(BF16)
    eight = iota((8, tokens), 0)
    keys_ref[...] = jnp.where(
        eight == 0, r0, jnp.where(eight == 1, r1, jnp.where(eight == 2, k0, k1))
    )
    cols_ref[...] = jnp.where(
        lane == 0, to_col(r0 * 8 + k0), jnp.where(lane == 1, to_col(r1 * 8 + k1), 0.0)
    )


def unpack_kernel(in_ref, out_ref):
    msgs = EXPERTS * 8
    p_row = iota((512, msgs), 0)
    p_col = iota((512, msgs), 1)
    chunk = p_row // 128
    half = (p_row % 128) // 64
    src = p_row % 64
    perm = onehot(p_col == src * 8 + half * 4 + chunk)
    rows = dot(perm, in_ref[...])
    by_src = rows[64:128, 256:384]
    tall = jnp.concatenate([by_src] * CAP, axis=0)
    t_row = iota((ROWS, 128), 0)
    t_lane = iota((ROWS, 128), 1)
    tall = jnp.where(t_row // 64 == t_lane, tall, 0.0).astype(BF16)
    w_row = dot_nt(jnp.full((EXTRA, 128), 1.0, BF16), tall).astype(BF16)
    rows = rows.astype(BF16)
    for t in range(TP):
        for c in range(4):
            for j in range(3):
                n = 128 if j < 2 else 64
                out_ref[t, j * 128 : j * 128 + n, c * 128 : (c + 1) * 128] = rows[
                    c * 128 : c * 128 + n, j * 128 : (j + 1) * 128
                ]
        out_ref[t, ROWS : ROWS + EXTRA, :] = jnp.zeros((EXTRA, 512), BF16)
        out_ref[t, ROWS : ROWS + EXTRA, 0:ROWS] = w_row


def expert_kernel(
    in_ref, wg_ref, wu_ref, wd_ref, z_ref, dg_out, du_out, wt_out, dg_ref, du_ref, wt_ref, sems
):
    outward = [
        pltpu.make_async_copy(src, dst, sems.at[n])
        for n, (src, dst) in enumerate(((dg_ref, dg_out), (du_ref, du_out), (wt_ref, wt_out)))
    ]

    def summed(lo, w_ref):
        return sum(
            dot_nt(in_ref[t, 0:ROWS, lo : lo + 256], w_ref[:, t * 256 : (t + 1) * 256])
            for t in range(TP)
        )

    pre_gate = summed(0, wg_ref)
    pre_up = summed(0, wu_ref)
    projected = summed(256, wd_ref)
    w_row = in_ref[0, ROWS : ROWS + EXTRA, 0:ROWS].astype(F32)[0:1, :]
    eye = iota((ROWS, ROWS), 0) == iota((ROWS, ROWS), 1)
    weight = jnp.sum(jnp.where(eye, w_row, 0.0), axis=1, keepdims=True)
    sig = jax.nn.sigmoid(pre_gate)
    activated = pre_gate * sig
    hidden = activated * pre_up
    route = jnp.sum(hidden.astype(BF16).astype(F32) * projected, axis=1, keepdims=True)
    grad = weight * projected
    d_gate = (grad * pre_up * sig * (1.0 + pre_gate * (1.0 - sig))).astype(BF16)
    d_up = (grad * activated).astype(BF16)
    dg_ref[...] = d_gate
    du_ref[...] = d_up
    wt_ref[...] = (weight * hidden).astype(BF16)
    for copy in outward:
        copy.start()
    part = (dot(d_gate, wg_ref[...]) + dot(d_up, wu_ref[...])).astype(BF16)
    hi = route.astype(BF16).astype(F32)
    lo = route - hi
    lane = iota((ROWS, 128), 1)
    pair = jnp.where(lane == 0, hi, jnp.where(lane == 1, lo, 0.0))
    pair = jnp.concatenate([pair, jnp.zeros((512 - ROWS, 128), F32)], axis=0).astype(BF16)
    pick = onehot(iota((EXTRA, 128), 0) == iota((EXTRA, 128), 1))
    flat = dot_nt(pick, pair)
    extra = jnp.concatenate([flat[0:8, 0:256], flat[0:8, 256:512]], axis=0).astype(BF16)
    for t in range(TP):
        z_ref[t, 0:ROWS, :] = part[:, t * 256 : (t + 1) * 256]
        z_ref[t, ROWS : ROWS + EXTRA, :] = extra
    for copy in outward:
        copy.wait()


def load_kernel(*refs):
    count = (len(refs) - 1) // 2
    copies = [
        pltpu.make_async_copy(refs[n], refs[count + n], refs[-1].at[n]) for n in range(count)
    ]
    for copy in copies:
        copy.start()
    for copy in copies:
        copy.wait()


def return_kernel(in_ref, out_ref):
    total = sum(in_ref[t].astype(F32) for t in range(TP))
    msgs = EXPERTS * 8
    rows = total[0:ROWS].astype(BF16)
    m_row = iota((msgs, 512), 0)
    m_col = iota((msgs, 512), 1)
    dest = m_row // 8
    sub = m_row % 8
    perm = onehot((m_col == sub * 64 + dest) & (sub < CAP))
    out = dot(perm[:, 0:ROWS], rows)
    first = total[ROWS : ROWS + 1] + total[ROWS + 1 : ROWS + 2]
    second = total[ROWS + 8 : ROWS + 9] + total[ROWS + 9 : ROWS + 10]
    route = jnp.concatenate([first, second], axis=1)
    hi = route.astype(BF16).astype(F32)
    lo = route - hi
    mine = (sub == CAP) & (m_col % 64 == dest)
    b_row = iota((512, 256), 0)
    b_col = iota((512, 256), 1)
    out = out + dot(jnp.where(mine, hi, 0.0).astype(BF16), onehot(b_row // 64 == b_col))
    out = out + dot(jnp.where(mine, lo, 0.0).astype(BF16), onehot(b_row // 64 == b_col - 128))
    mix = total[ROWS + 2 : ROWS + 3, 0:128] + total[ROWS + 3 : ROWS + 4, 0:128]
    mix_hi = mix.astype(BF16).astype(F32)
    mix_row = jnp.concatenate([mix_hi, mix - mix_hi], axis=1)
    out_sub = iota((msgs, 256), 0) % 8
    out = jnp.where(out_sub == CAP + 1, mix_row, out)
    out_ref[...] = out.astype(BF16)


def final_kernel(in_ref, keys_ref, cols_ref, dense_ref, tok_ref, route_ref, mix_ref):
    msgs = EXPERTS * 8
    got = in_ref[...]
    lane = iota((128, msgs), 1).astype(F32)
    take = onehot((lane == cols_ref[:, 0:1]) | (lane == cols_ref[:, 1:2]))
    tok_ref[...] = (dot(take, got) + dense_ref[...]).astype(BF16)
    m_row = iota((msgs, 128), 0).astype(F32)
    l_row = iota((256, 128), 0).astype(F32)
    for a in range(2):
        expert = keys_ref[a : a + 1, :]
        rank = keys_ref[a + 2 : a + 3, :]
        cells = dot_tn(got, onehot(m_row == expert * 8 + CAP))
        keep = (l_row == rank) | (l_row == rank + 128)
        route_ref[a : a + 1, :] = jnp.sum(jnp.where(keep, cells, 0.0), axis=0, keepdims=True)
    e_row = iota((EXPERTS, msgs), 0)
    e_col = iota((EXPERTS, msgs), 1)
    mix = dot(onehot(e_col == peer_of(e_row) * 8 + CAP + 1), got)
    mix_ref[...] = mix[:, 0:128] + mix[:, 128:256]


def moment_kernel(cot_ref, tok_ref, out_ref):
    moment = dot_tn(cot_ref[...], tok_ref[...])
    for x in range(4):
        starts = [(z * 8 + x * 2) * 8 for z in range(16)]
        out_ref[x * 256 : (x + 1) * 256, :] = jnp.concatenate(
            [moment[s : s + 16] for s in starts], axis=0
        )


def core_sum_kernel(keep_ref, got_ref, own_ref, s1_ref, s2_ref, s3_ref, sum_ref):
    sum_ref[...] = keep_ref[...] + got_ref[...]
    here = lax.axis_index("ep_1")

    def part(shift):
        start = pl.multiple_of(lax.rem(here + shift, 4) * 256, 256)
        return sum_ref[pl.ds(start, 256), :]

    own_ref[...] = part(0)
    s1_ref[...] = part(1).astype(BF16)
    s2_ref[...] = part(2).astype(BF16)
    s3_ref[...] = part(3).astype(BF16)


def x_sum_kernel(own_ref, r1_ref, r2_ref, r3_ref, dense_ref, out_ref):
    total = own_ref[...] + r1_ref[...].astype(F32)
    total = total + (r2_ref[...].astype(F32) + r3_ref[...].astype(F32))
    dense = dense_ref[...].astype(F32)
    pieces = []
    for z in range(16):
        pieces += [total[z * 16 : z * 16 + 16], dense]
    out_ref[...] = jnp.concatenate(pieces, axis=0).astype(BF16)


def z_sum_kernel(in_ref, gate_ref, dense_ref, dense_other_ref, grad_ref, share_ref, w_ref):
    got = in_ref[...].astype(F32)
    moment = sum(got[z * 24 : z * 24 + 16] for z in range(16)) * (1.0 / 128)
    w_ref[...] = jnp.concatenate(
        [got[z * 24 + 16 : z * 24 + 24] for z in range(16)], axis=0
    ).astype(BF16)
    core = lax.axis_index("ep_2")
    first = (lax.axis_index("ep_0") * 8 + lax.axis_index("ep_1") * 2 + core) * 8
    at = iota((8, 1024), 1) == first + iota((8, 1024), 0)
    gate = jnp.sum(jnp.where(at, gate_ref[...], 0.0), axis=1, keepdims=True)
    grad_ref[...] = jnp.where(core == 0, moment[0:8], moment[8:16]) * gate
    own = dense_ref[...].astype(F32)
    other = dense_other_ref[...].astype(F32)
    dense = jnp.concatenate(
        [jnp.where(core == 0, own, other), jnp.where(core == 0, other, own)], axis=0
    )
    share = jnp.sum(moment * dense, axis=1, keepdims=True)
    spot = iota((16, 128), 1) == iota((16, 128), 0)
    row = jnp.sum(jnp.where(spot, share, 0.0), axis=0, keepdims=True)
    share_ref[...] = jnp.broadcast_to(row, (8, 128))


def dense_kernel(cot_ref, gate_ref, own_ref, other_ref, out_ref):
    north = lax.axis_index("ep_2") == 1
    own = own_ref[...].astype(F32)
    other = other_ref[...].astype(F32)
    south_w = jnp.where(north, other, own)
    north_w = jnp.where(north, own, other)
    pieces = []
    for z in range(16):
        for x in range(4):
            s = (x * 16 + z) * 8
            pieces += [south_w[s : s + 8], north_w[s : s + 8]]
    weight = jnp.concatenate(pieces, axis=0).astype(BF16)
    scaled = (gate_ref[...] * cot_ref[...].astype(F32)).astype(BF16)
    out_ref[...] = dot(scaled, weight)


def add_kernel(a_ref, b_ref, mix_ref, out_ref):
    def parts(value):
        hi = value.astype(BF16).astype(F32)
        return hi, value - hi

    mix = parts(jnp.concatenate([mix_ref[0:1, :], jnp.zeros((1, 128), F32)], axis=1))
    sub = iota((8, 256), 0)
    extra = []
    both = a_ref[0, ROWS : ROWS + EXTRA, :].astype(F32) + b_ref[0, ROWS : ROWS + EXTRA, :].astype(F32)
    for at in (0, 8):
        block = jnp.zeros((8, 256), F32)
        for n, row in enumerate(parts(both[at : at + 1] + both[at + 1 : at + 2]) + mix):
            block = jnp.where(sub == n, row, block)
        extra.append(block)
    extra = jnp.concatenate(extra, axis=0).astype(BF16)
    for t in range(TP):
        total = a_ref[t, 0:ROWS, :].astype(F32) + b_ref[t, 0:ROWS, :].astype(F32)
        out_ref[t, 0:ROWS, :] = total.astype(BF16)
        out_ref[t, ROWS : ROWS + EXTRA, :] = extra


def in_place(*arrays):
    return [pltpu.with_memory_space_constraint(a, pltpu.HBM) for a in arrays]


def swap(value, axes):
    return lax.all_to_all(value, axes, split_axis=0, concat_axis=0, tiled=True)


def shift(value, axis, by):
    n = lax.axis_size(axis)
    return lax.ppermute(value, axis, [(i, (i + by) % n) for i in range(n)])


def local(tokens, cotangent, routes, route_weights, w_gate, w_up, w_down, dense_weight, mix_gate):
    wg = w_gate[0].T
    wu = w_up[0].T
    wd = w_down[0]
    dense_t = dense_weight.T
    gate_row = mix_gate[None, :]
    tokens, cotangent, wg, wu, wd, routes_t, weights_t = in_place(
        tokens, cotangent, wg, wu, wd, routes.T, route_weights.T
    )
    packed, keys, cols, cot_here = call(
        pack_kernel,
        (
            struct(512, 384),
            struct(8, 128, dtype=F32),
            struct(128, 128, dtype=F32),
            struct(128, 256),
        ),
        tokens,
        cotangent,
        routes_t,
        weights_t,
    )
    arrived = swap(packed.reshape(64, 8, 384), CHIPS)

    cot_all = lax.all_gather(cot_here, "tp", axis=1, tiled=True)
    dense_other = shift(lax.optimization_barrier((dense_t, cot_all))[0], "ep_2", 1)
    keep = call(moment_kernel, struct(1024, 256, dtype=F32), cot_all, tokens)
    here, *away = call(
        core_sum_kernel,
        (struct(256, 256, dtype=F32),) + (struct(256, 256),) * 3,
        keep,
        shift(keep, "ep_2", 1),
        scratch=(pltpu.VMEM((1024, 256), F32),),
        after=(dense_other,),
    )
    both = call(
        x_sum_kernel,
        struct(384, 256),
        here,
        *(shift(piece, "ep_1", i + 1) for i, piece in enumerate(away)),
        dense_t,
    )

    own = call(
        unpack_kernel, struct(TP, ROWS + EXTRA, 512), arrived.reshape(512, 384), after=(here,)
    )
    own, both = lax.optimization_barrier((swap(own, "tp"), both))
    other = shift(own, "ep_2", 1)
    outs = (struct(TP, ROWS + EXTRA, 256),) + (pltpu.HBM((ROWS, 352), BF16),) * 3
    hbm_spec = pl.BlockSpec(memory_space=pltpu.HBM)
    vmem_spec = pl.BlockSpec(memory_space=pltpu.VMEM)
    expert = dict(
        flops=1_150_000_000,
        out_specs=(vmem_spec,) + (hbm_spec,) * 3,
        scratch=(pltpu.VMEM((ROWS, 352), BF16),) * 3 + (pltpu.SemaphoreType.DMA((3,)),),
    )
    weights = call(
        load_kernel,
        (struct(352, 1024),) * 3,
        wg,
        wu,
        wd,
        hbm=3,
        scratch=(pltpu.SemaphoreType.DMA((3,)),),
    )
    z_own, *act_own = call(expert_kernel, outs, own, *weights, **expert)
    z_got = swap(both.reshape(16, 24, 256), "ep_0").reshape(384, 256)
    z_other, *act_other = call(expert_kernel, outs, other, *weights, **expert)
    z_back = shift(z_other, "ep_2", 1)
    z_back, z_got = lax.optimization_barrier((z_back, z_got))
    dense_grad, share, dense_w = call(
        z_sum_kernel,
        (struct(8, 256, dtype=F32), struct(8, 128, dtype=F32), struct(128, 256)),
        z_got,
        gate_row,
        dense_t,
        dense_other,
    )
    z_sum = call(add_kernel, outs[0], z_own, z_back, share)
    z_all = swap(z_sum, "tp")
    dense_w = lax.all_gather(dense_w, "ep_1", axis=0, tiled=True)
    z_all, dense_w = lax.optimization_barrier((z_all, dense_w))
    back_ready = call(return_kernel, struct(512, 256), z_all)
    gate_grad, up_grad, down_grad, grads_done = call(
        grads_kernel,
        (struct(352, 1024),) * 3 + (struct(8, 128, dtype=F32),),
        own,
        other,
        *in_place(*act_own, *act_other),
        after=(back_ready,),
        scratch=(pltpu.VMEM((352, 1024), BF16),) * 3 + (pltpu.SemaphoreType.DMA((3,)),),
        out_specs=(hbm_spec,) * 3 + (vmem_spec,),
        flops=1_400_000_000,
    )
    back = swap(back_ready.reshape(64, 8, 256), CHIPS).reshape(512, 256)

    dense_dx = call(
        dense_kernel,
        struct(128, 256, dtype=F32),
        cot_all,
        gate_row,
        dense_w,
        shift(dense_w, "ep_2", 1),
    )
    token_grad, route_t, mix_all = call(
        final_kernel,
        (struct(128, 256), struct(2, 128, dtype=F32), struct(EXPERTS, 128, dtype=F32)),
        back,
        keys,
        cols,
        dense_dx,
        after=(grads_done,),
    )
    mix_grad = mix_all[:, :16].reshape(1024)
    return (
        token_grad,
        route_t.T,
        gate_grad.T[None],
        up_grad.T[None],
        down_grad[None],
        dense_grad.T,
        mix_grad,
    )


def grads_kernel(
    own_ref, other_ref, dg0, du0, wt0, dg1, du1, wt1,
    gate_ref, up_ref, down_ref, done_ref, gate_tmp, up_tmp, down_tmp, sems,
):
    copies = []
    for n, (left0, left1, lo, out_ref, tmp) in enumerate((
        (dg0, dg1, 0, gate_ref, gate_tmp),
        (du0, du1, 0, up_ref, up_tmp),
        (wt0, wt1, 256, down_ref, down_tmp),
    )):
        left = jnp.concatenate([left0[...], left1[...]], axis=0)
        for t in range(TP):
            right = jnp.concatenate(
                [own_ref[t, 0:ROWS, lo : lo + 256], other_ref[t, 0:ROWS, lo : lo + 256]], axis=0
            )
            tmp[:, t * 256 : (t + 1) * 256] = dot_tn(left, right).astype(BF16)
        copies.append(pltpu.make_async_copy(tmp, out_ref, sems.at[n]))
        copies[-1].start()
    done_ref[...] = jnp.zeros((8, 128), F32)
    for copy in copies:
        copy.wait()


def solution(mesh):
    finer = Mesh(mesh.devices.reshape(16, 4, 2, mesh.shape["tp"]), ("ep_0", "ep_1", "ep_2", "tp"))
    in_specs = (
        P(EP, "tp"),
        P(EP, "tp"),
        P(EP, None),
        P(EP, None),
        P(EP, None, "tp"),
        P(EP, None, "tp"),
        P(EP, "tp", None),
        P("tp", EP),
        P(),
    )
    out_specs = (
        P(EP, "tp"),
        P(EP, None),
        P(EP, None, "tp"),
        P(EP, None, "tp"),
        P(EP, "tp", None),
        P("tp", EP),
        P(),
    )
    return jax.shard_map(local, mesh=finer, in_specs=in_specs, out_specs=out_specs, check_vma=False)
```
